256 devices in a mesh: ep: 64 (over z, x, core), tp: 4 (over y).
Axes of the slice: x: 4, y: 4, z: 8, core: 2. Of those that a mesh axis runs over, the one named last changes fastest.
Arguments:
- query_rows: bfloat16 [16384, 1024], P('ep', 'tp'), may hold values from -8 to 8
- key_rows: bfloat16 [16384, 256], P('ep', 'tp'), may hold values from -8 to 8
- value_rows: bfloat16 [16384, 256], P('ep', 'tp'), may hold values from -16 to 16
- query_gain: float32 [64], replicated, may hold values from 0.5 to 7.5
- key_gain: float32 [64], replicated, may hold values from 0.5 to 7.5
- moe_tokens: bfloat16 [32768, 2048], P(('ep', 'tp')), may hold values from -6 to 6
- norm_gain: float32 [2048], replicated, may hold values from 0.1 to 1.9
- routes: int32 [32768, 2], P('ep'), may hold values from 0 to 63, all different within a row; in each aligned block of 128 rows (0 to 127, 128 to 255, ...) at most 8 rows name the same one
- route_weights: float32 [32768, 2], P('ep'), may hold values from 0.1 to 1
- expert_gate: bfloat16 [64, 2048, 1024], P('ep', None, 'tp'), may hold values from -0.125 to 0.125
- expert_up: bfloat16 [64, 2048, 1024], P('ep', None, 'tp'), may hold values from -0.125 to 0.125
- expert_down: bfloat16 [64, 1024, 2048], P('ep', 'tp'), may hold values from -0.1875 to 0.1875
- shared_gate: bfloat16 [2048, 1024], P(None, 'tp'), may hold values from -0.125 to 0.125
- shared_up: bfloat16 [2048, 1024], P(None, 'tp'), may hold values from -0.125 to 0.125
- shared_down: bfloat16 [1024, 2048], P('tp'), may hold values from -0.1875 to 0.1875
Outputs:
- attn_out: bfloat16 [16384, 1024], P('ep', 'tp')
- moe_out: bfloat16 [32768, 2048], P(('ep', 'tp'))
The draws below stay inside these ranges and needn't reach their ends.
Inputs may be any that keep to these rules, and one draw needn't show every extreme that they name: `routes`: each row names 2 different experts. Within each aligned block of 128 rows no expert is named more than 8 times, and in every draw some expert is named exactly 8 times in some block.
All inputs are finite; a program needn't handle non-finite values.
Results may differ from the reference program's by a relative error of at most 0.012.
The reference program's roundings to bfloat16 on the way count: a program that leaves them out, or rounds other values in their place, can miss the bound.
Values may be sent and summed in bfloat16 or wider, within the bound.
A program may use at most 192 MiB of HBM per device.

```python
import math
import jax
import jax.numpy as jnp
import numpy as np
from jax import lax

D = 2048
HEADS = 16
KV_HEADS = 4
HD = 64
F = 1024
TOP = 2
GRID_W = 64
TOK_B = 128
TOKENS_A = 16384
TOKENS_B = 32768
EXPERTS = 64
CAP = 8
N_TP = 4


def draw_key_rows(key, part):
    result = jnp.clip(jax.random.normal(jax.random.fold_in(key, 72), (TOKENS_A, KV_HEADS * HD), jnp.float32), -6.0, 6.0)
    return result.astype(jnp.bfloat16)


def draw_query_rows(key, part):
    result = jnp.clip(jax.random.normal(jax.random.fold_in(key, 73), (TOKENS_A, HEADS * HD), jnp.float32), -6.0, 6.0)
    return result.astype(jnp.bfloat16)


def gain_draw(key, salt):
    result = jax.random.uniform(jax.random.fold_in(key, salt + 3), (HD,), jnp.float32, 1.2, 1.8)
    return result


def draw_query_gain(key, part):
    return gain_draw(key, 80)


def draw_key_gain(key, part):
    return gain_draw(key, 90)


def level_of(key, dims, pieces, low, top_value):
    factor_of, own = 1.0, jax.random.fold_in(key, 6)
    for axis_at, blocks in pieces:
        heights = jnp.exp(jax.random.uniform(jax.random.fold_in(own, axis_at), (blocks,), jnp.float32, low / len(pieces), top_value / len(pieces)))
        factor_of = factor_of * jnp.repeat(heights, dims[axis_at] // blocks).reshape([-1 if axis == axis_at else 1 for axis in range(len(dims))])
    return factor_of


def assign_block(stream_key, own, number, rows, amount, top, bound, slope):
    ranking = jax.random.permutation(stream_key, amount)
    crowded, common = portions_of(amount, rows * top, bound, slope, True), portions_of(amount, rows * top, bound, slope, False)
    places = jnp.arange(amount)

    def named(sizes, rotation):
        used = int((sizes > 0).sum())
        fixed = max(1, used // 4)
        passed = fixed + (places - fixed + rotation * (used - fixed)) % max(1, amount - fixed)
        return jnp.zeros((amount,), jnp.int32).at[ranking[jnp.where(places < fixed, places, passed)]].set(jnp.asarray(sizes, jnp.int32))

    sizes = jnp.where(number % 4 == 0, named(crowded, number // 4), named(common, number - number // 4 - 1))
    mixed = jax.random.permutation(jax.random.fold_in(own, 3), amount)
    source_of, receiver = mixed[0:amount // 2 * 2:2], mixed[1:amount // 2 * 2:2]
    room = jnp.minimum(sizes[source_of] - 1, bound - sizes[receiver]) // 2
    room = jnp.where((source_of == ranking[0]) | (receiver == ranking[0]) | (sizes[receiver] == 0), 0, jnp.maximum(room, 0))
    passed = jax.random.randint(jax.random.fold_in(own, 4), (amount // 2,), 0, 1 << 20) % (room + 1)
    sizes = sizes.at[source_of].add(-passed).at[receiver].add(passed)
    items = jnp.searchsorted(jnp.cumsum(sizes), jnp.arange(rows * top), side="right").astype(jnp.int32)
    table = items.reshape(top, rows).T
    table = table[jax.random.permutation(jax.random.fold_in(own, 1), rows)]
    rotation = jax.random.randint(jax.random.fold_in(own, 2), (rows, 1), 0, top)
    return jnp.take_along_axis(table, (jnp.arange(top)[None, :] + rotation) % top, axis=1)


def portions_of(number_of, total, limit, skew, full):
    weights = [(1 << 20) // math.isqrt(standing ** skew) + 1 for standing in range(1, number_of + 1)]
    largest = limit if full else min(limit, max(-(-total // number_of), total * weights[0] // sum(weights)))
    least = 1 if total - largest >= number_of - 1 else 0
    holding, surplus = [largest] + [least] * (number_of - 1), total - largest - least * (number_of - 1)
    while surplus > 0:
        movable = [i for i in range(1, number_of) if holding[i] < largest] or [i for i in range(1, number_of) if holding[i] < limit]
        pool, remaining = sum([weights[i] for i in movable]), surplus
        for i in movable:
            more = min(limit - holding[i], max(1, remaining * weights[i] // pool), surplus)
            holding[i] = holding[i] + more
            surplus = surplus - more
    return np.array(holding)


def gaussian(key, extent, width, reach, pieces=(), kind=jnp.bfloat16):
    entries = width * jax.random.normal(key, extent, jnp.float32)
    if pieces:
        entries = entries * level_of(key, extent, pieces, -0.22, 0.18)
    return jnp.clip(entries, -reach, reach).astype(kind)


def setup_inputs(seed: int = 0) -> dict:
    key_list = jax.random.split(jax.random.key(seed), 16)
    query_rows = draw_query_rows(jax.random.fold_in(key_list[15], 71), 0)
    key_rows = draw_key_rows(jax.random.fold_in(key_list[15], 71), 0)
    value_rows = gaussian(key_list[2], (TOKENS_A, KV_HEADS * HD), 3.0, 16.0, ((0, 64), (1, 4)))
    query_gain = draw_query_gain(jax.random.fold_in(key_list[15], 71), 0)
    key_gain = draw_key_gain(jax.random.fold_in(key_list[15], 71), 0)
    moe_tokens = gaussian(key_list[5], (TOKENS_B, D), 1.0, 6.0, ((0, 256),))
    norm_gain = jnp.clip(1.0 + 0.18 * jax.random.normal(key_list[6], (D,), jnp.float32), 0.1, 1.9)
    routes_keys = jax.random.split(jax.random.fold_in(key_list[7], 1), TOKENS_B // TOK_B)
    routes_turns = jax.random.permutation(jax.random.fold_in(key_list[7], 3), TOKENS_B // TOK_B)
    routes = jax.vmap(lambda own, number: assign_block(jax.random.fold_in(key_list[7], 2), own, number, TOK_B, EXPERTS, TOP, CAP, 1))(routes_keys, routes_turns).reshape((TOKENS_B, TOP))
    route_weights = jnp.clip(0.1 + 0.9 * jax.random.uniform(key_list[8], (TOKENS_B, TOP), jnp.float32) ** level_of(key_list[8], (TOKENS_B, TOP), ((0, 64),), -0.2, 0.2), 0.1, 1.0)
    expert_gate = gaussian(key_list[9], (EXPERTS, D, F), D ** -0.5, 0.125, ((0, 64), (2, 4)))
    expert_up = gaussian(key_list[10], (EXPERTS, D, F), D ** -0.5, 0.125, ((0, 64), (2, 4)))
    expert_down = gaussian(key_list[11], (EXPERTS, F, D), F ** -0.5, 0.1875, ((0, 64), (1, 4)))
    shared_gate = gaussian(key_list[12], (D, F), D ** -0.5, 0.125, ((1, 4),))
    shared_up = gaussian(key_list[13], (D, F), D ** -0.5, 0.125, ((1, 4),))
    shared_down = gaussian(key_list[14], (F, D), F ** -0.5, 0.1875, ((0, 4),))
    return {"query_rows": query_rows, "key_rows": key_rows, "value_rows": value_rows, "query_gain": query_gain, "key_gain": key_gain, "moe_tokens": moe_tokens, "norm_gain": norm_gain, "routes": routes, "route_weights": route_weights, "expert_gate": expert_gate, "expert_up": expert_up, "expert_down": expert_down, "shared_gate": shared_gate, "shared_up": shared_up, "shared_down": shared_down}


epsilon = 1e-06
rotary_base = 10000.0
routed_scale = 2.5

def rotate_heads(heads_in, gain_row, positions):
    values32 = heads_in.astype(jnp.float32)
    scaled = values32 * lax.rsqrt(lax.optimization_barrier(jnp.mean(values32 * values32, axis=-1, keepdims=True)) + epsilon) * gain_row
    pair_count = scaled.shape[-1] // 4
    inv_freq = rotary_base ** (-jnp.arange(pair_count, dtype=jnp.float32) / pair_count)
    grid_row = (positions // GRID_W).astype(jnp.float32)
    grid_col = (positions % GRID_W).astype(jnp.float32)
    angles = jnp.concatenate([grid_row[:, None] * inv_freq, grid_col[:, None] * inv_freq], axis=-1)[:, None, :]
    cosine = jnp.cos(angles)
    sine_part = jnp.sin(angles)
    first_half = scaled[..., 0::2]
    second_half = scaled[..., 1::2]
    turned = jnp.stack([first_half * cosine - second_half * sine_part, first_half * sine_part + second_half * cosine], axis=-1)
    return turned.reshape(scaled.shape).astype(jnp.bfloat16)

def attention(query_rows, key_rows, value_rows, query_gain, key_gain):
    token_count = query_rows.shape[0]
    group = HEADS // KV_HEADS
    positions = jnp.arange(token_count, dtype=jnp.int32)
    q_rot = rotate_heads(query_rows.reshape(token_count, HEADS, HD), query_gain, positions)
    k_rot = rotate_heads(key_rows.reshape(token_count, KV_HEADS, HD), key_gain, positions)
    keys32 = lax.optimization_barrier(k_rot).astype(jnp.float32)
    values32 = value_rows.reshape(token_count, KV_HEADS, HD).astype(jnp.float32)
    block_len = math.gcd(token_count, 256)
    q_blocks = lax.optimization_barrier(q_rot).reshape(token_count // block_len, block_len, KV_HEADS, group, HD)

    def one_block(q_block):
        scores = jnp.einsum('qgrd,sgd->qgrs', q_block.astype(jnp.float32), keys32) * HD ** (-0.5)
        row_max = lax.optimization_barrier(jnp.max(scores, axis=-1, keepdims=True))
        weights = jnp.exp(scores - row_max)
        row_sum = lax.optimization_barrier(jnp.sum(weights, axis=-1, keepdims=True))
        rounded = lax.optimization_barrier(weights.astype(jnp.bfloat16)).astype(jnp.float32)
        mixed = jnp.einsum('qgrs,sgd->qgrd', rounded, values32)
        return (mixed / row_sum).astype(jnp.bfloat16)
    result = lax.map(one_block, q_blocks)
    return result.reshape(token_count, HEADS * HD)

def feed_forward(rows_in, w_gate, w_up, w_down):
    gate_proj = jnp.dot(rows_in, w_gate, preferred_element_type=jnp.float32)
    up_proj = jnp.dot(rows_in, w_up, preferred_element_type=jnp.float32)
    hidden = lax.optimization_barrier((jax.nn.silu(gate_proj) * up_proj).astype(jnp.bfloat16))
    block_width = hidden.shape[-1] // N_TP
    summed = jnp.zeros((rows_in.shape[0], w_down.shape[1]), jnp.float32)
    for part_index in range(N_TP):
        lower = part_index * block_width
        partial_sum = jnp.dot(hidden[:, lower:lower + block_width], w_down[lower:lower + block_width], preferred_element_type=jnp.float32).astype(jnp.bfloat16)
        summed = summed + lax.optimization_barrier(partial_sum).astype(jnp.float32)
    return summed

def mixture(moe_tokens, norm_gain, routes, route_weights, expert_gate, expert_up, expert_down, shared_gate, shared_up, shared_down):
    total_rows = moe_tokens.shape[0]
    blocks = total_rows // TOK_B
    values32 = moe_tokens.astype(jnp.float32)
    normed = (values32 * lax.rsqrt(lax.optimization_barrier(jnp.mean(values32 * values32, axis=-1, keepdims=True)) + epsilon) * norm_gain).astype(jnp.bfloat16)
    normed = lax.optimization_barrier(normed)
    gates = route_weights / lax.optimization_barrier(jnp.sum(route_weights, axis=-1, keepdims=True)) * routed_scale
    chosen = routes.reshape(blocks, TOK_B * TOP).astype(jnp.int32)
    one_hot = (chosen[:, :, None] == jnp.arange(EXPERTS, dtype=jnp.int32)[None, None, :]).astype(jnp.int32)
    ranks = lax.optimization_barrier(jnp.sum((jnp.cumsum(one_hot, axis=1) - one_hot) * one_hot, axis=2))
    block_ids = jnp.arange(blocks, dtype=jnp.int32)[:, None]
    dest = (chosen * blocks + block_ids) * CAP + ranks
    rows_from = block_ids * TOK_B + jnp.arange(TOK_B * TOP, dtype=jnp.int32)[None, :] // TOP
    slot_rows = jnp.full((EXPERTS * blocks * CAP,), total_rows, jnp.int32).at[dest.reshape(-1)].set(rows_from.reshape(-1))
    padded = jnp.concatenate([normed, jnp.zeros((1, D), jnp.bfloat16)], axis=0)

    def one_expert(inputs):
        index_rows, w_gate, w_up, w_down = inputs
        return feed_forward(padded[index_rows], w_gate, w_up, w_down).astype(jnp.bfloat16)
    expert_rows = lax.map(one_expert, (slot_rows.reshape(EXPERTS, blocks * CAP), expert_gate, expert_up, expert_down))
    flat_rows = lax.optimization_barrier(expert_rows.reshape(EXPERTS * blocks * CAP, D))
    picked = flat_rows[dest.reshape(-1)].astype(jnp.float32).reshape(total_rows, TOP, D)
    routed = lax.optimization_barrier(jnp.sum(gates[:, :, None] * picked, axis=1))
    shared = feed_forward(normed, shared_gate, shared_up, shared_down)
    return (routed + shared).astype(jnp.bfloat16)

def reference(query_rows, key_rows, value_rows, query_gain, key_gain, moe_tokens, norm_gain, routes, route_weights, expert_gate, expert_up, expert_down, shared_gate, shared_up, shared_down):
    attn_out = attention(query_rows, key_rows, value_rows, query_gain, key_gain)
    moe_out = mixture(moe_tokens, norm_gain, routes, route_weights, expert_gate, expert_up, expert_down, shared_gate, shared_up, shared_down)
    return (attn_out, moe_out)
```

```python
import functools

import jax
import jax.numpy as jnp
from jax import lax
from jax.experimental import pallas as pl
from jax.experimental.pallas import tpu as pltpu
from jax.sharding import PartitionSpec as P

GRID_W = 64
MESH = pl.DeviceIdType.MESH
F32 = jnp.float32
BF16 = jnp.bfloat16

epsilon = 1e-06
rotary_base = 10000.0
routed_scale = 2.5

N_Z, N_X, N_CORE = 8, 4, 2
N_EP, N_TP = 64, 4
CAP = 8
CHUNKS = 4
NT = (((1,), (1,)), ((), ()))


def prep_kernel(q_ref, kv_ref, qg_ref, kg_ref, cos_ref, sin_ref, qo_ref, kvo_ref):
    rows = q_ref.shape[0]
    lane = lax.broadcasted_iota(jnp.int32, (rows, 128), 1)
    low = lane < 64
    even = lax.rem(lane, 2) == 0
    cosine, sine = cos_ref[...], sin_ref[...]

    def turned(x, gain):
        squares = x * x
        first = jnp.sum(jnp.where(low, squares, 0.0), axis=1, keepdims=True) / 64.0
        second = jnp.sum(jnp.where(low, 0.0, squares), axis=1, keepdims=True) / 64.0
        inverse = jnp.where(low, lax.rsqrt(first + epsilon), lax.rsqrt(second + epsilon))
        y = x * inverse * gain
        partner = jnp.where(even, -pltpu.roll(y, 127, 1), pltpu.roll(y, 1, 1))
        return (y * cosine + partner * sine).astype(BF16).astype(F32)

    gain = qg_ref[...]
    for pair in range(q_ref.shape[1] // 128):
        x = q_ref[:, pair * 128 : pair * 128 + 128].astype(F32)
        out = turned(x, gain) * 0.125
        base = 2 * pair * rows
        qo_ref[base : base + rows, :] = jnp.where(low, out, 0.0).astype(BF16)
        qo_ref[base + rows : base + 2 * rows, :] = jnp.where(
            low, pltpu.roll(out, 64, 1), 0.0
        ).astype(BF16)
    kv = kv_ref[...].astype(F32)
    kvo_ref[...] = jnp.where(low, turned(kv, kg_ref[...]), kv).astype(BF16)


def prepared(query_rows, key_rows, value_rows, query_gain, key_gain):
    rows = query_rows.shape[0]
    positions = lax.axis_index("ep") * rows + jnp.arange(rows, dtype=jnp.int32)
    pair_count = 16
    inv_freq = rotary_base ** (-jnp.arange(pair_count, dtype=F32) / pair_count)
    grid_row = (positions // GRID_W).astype(F32)
    grid_col = (positions % GRID_W).astype(F32)
    angles = jnp.concatenate([grid_row[:, None] * inv_freq, grid_col[:, None] * inv_freq], axis=-1)
    angles = jnp.tile(jnp.repeat(angles, 2, axis=1), (1, 2))
    kv = jnp.concatenate([key_rows, value_rows], axis=1)
    return pl.pallas_call(
        prep_kernel,
        out_shape=[
            jax.ShapeDtypeStruct((4 * rows, 128), BF16),
            jax.ShapeDtypeStruct((rows, 128), BF16),
        ],
        name="prep",
    )(
        query_rows,
        kv,
        jnp.tile(query_gain[None, :], (1, 2)),
        jnp.tile(key_gain[None, :], (1, 2)),
        jnp.cos(angles),
        jnp.sin(angles),
    )


def silu_times(gate, up):
    return (gate / (1.0 + jnp.exp(-gate)) * up).astype(BF16)


def layer_kernel(
    q_ref, kv_ref, send_ref, normed_ref, choose_ref, gates_ref,
    wg_ref, wu_ref, wd_ref, sg_ref, su_ref, sd_ref,
    attn_ref, moe_ref,
    kvb, run_max, run_sum, mixed,
    wgb, wub, wdb, nall, arrived, rows_bf, hidden, outbuf, ret,
    sgb, sub, sdb, part, parts,
    item_send, item_recv, kv_send, kv_recv, x_send, x_recv, core_send, core_recv,
    disp_send, disp_recv, ret_send, ret_recv, rs_send, rs_recv, own_sem,
):
    me, lane = lax.axis_index("ep"), lax.axis_index("tp")
    z, x, c = lax.div(me, 8), lax.rem(lax.div(me, 2), 4), lax.rem(me, 2)
    right, left = lax.rem(lane + 1, N_TP), lax.rem(lane + 3, N_TP)
    opposite = lax.rem(lane + 2, N_TP)

    def at(zz, xx, cc):
        return (zz * N_X + xx) * N_CORE + cc

    def remote(src, dst, send_sem, recv_sem, axis, peer):
        return pltpu.make_async_remote_copy(
            src_ref=src, dst_ref=dst, send_sem=send_sem, recv_sem=recv_sem,
            device_id={axis: peer}, device_id_type=MESH,
        )

    barrier = pltpu.get_barrier_semaphore()

    def greet(i, carry):
        pl.semaphore_signal(
            barrier, inc=1, device_id={"ep": lax.rem(me + i, N_EP)}, device_id_type=MESH
        )
        return carry

    for i in range(1, N_TP):
        pl.semaphore_signal(
            barrier, inc=1, device_id={"tp": lax.rem(lane + i, N_TP)}, device_id_type=MESH
        )
    lax.fori_loop(1, N_EP, greet, 0)
    pl.semaphore_wait(barrier, N_EP - 1 + N_TP - 1)

    items = []
    for ref, buf in ((wg_ref, wgb), (wu_ref, wub)):
        for h in range(2):
            items.append((ref.at[pl.ds(h * 1024, 1024)], buf, (pl.ds(h * 1024, 1024),), h * 1024, 512))
    for j in range(CHUNKS):
        items.append((wd_ref.at[:, pl.ds(j * 512, 512)], wdb, (j,), 0, 128))
    items.append((normed_ref, nall, (), 0, 64))

    def item_copy(i, n):
        src, buf, where, base, half = items[i]
        lead = where[:-1] if where and not isinstance(where[0], int) else where
        s, r = item_send.at[i], item_recv.at[i]
        lower, upper = pl.ds(base, half), pl.ds(base + half, half)

        def piece(slot, rows):
            return buf.at[(slot,) + lead + (rows,)]

        if n == 0:
            return remote(src, buf.at[(1,) + where], s.at[0], r.at[0], "tp", right)
        if n == 1:
            return remote(src, buf.at[(2,) + where], s.at[1], r.at[1], "tp", left)
        if n == 2:
            return remote(piece(1, lower), piece(3, lower), s.at[2], r.at[2], "tp", right)
        return remote(piece(2, upper), piece(3, upper), s.at[3], r.at[3], "tp", left)

    def begin(i):
        if i < len(items):
            item_copy(i, 0).start()
            item_copy(i, 1).start()

    def service(i):
        item_copy(i, 0).wait_recv()
        item_copy(i, 2).start()
        item_copy(i, 1).wait_recv()
        item_copy(i, 3).start()
        begin(i + 2)

    def complete(i):
        item_copy(i, 2).wait_recv()
        item_copy(i, 3).wait_recv()

    begin(0)
    begin(1)

    local = [pltpu.make_async_copy(kv_ref, kvb.at[c, x, z], own_sem.at[0])]
    for n, (src, dst) in enumerate((
        (wg_ref, wgb.at[0]), (wu_ref, wub.at[0]), (sg_ref, sgb), (su_ref, sub), (sd_ref, sdb),
        (normed_ref, nall.at[0]), (send_ref.at[me], arrived.at[me]),
    )):
        local.append(pltpu.make_async_copy(src, dst, own_sem.at[n + 1]))
    for j in range(CHUNKS):
        local.append(pltpu.make_async_copy(
            wd_ref.at[:, pl.ds(j * 512, 512)], wdb.at[0, j], own_sem.at[8 + j]
        ))

    def along_z(i):
        return remote(
            kv_ref, kvb.at[c, x, z], kv_send.at[i], kv_recv.at[i],
            "ep", at(lax.rem(z + i, N_Z), x, c),
        )

    local[0].start()
    for i in range(1, N_Z):
        along_z(i).start()
    for copy in local[1:]:
        copy.start()

    x_next, x_prev = lax.rem(x + 1, N_X), lax.rem(x + 3, N_X)
    x_far = lax.rem(x + 2, N_X)
    up_x, down_x = at(z, x_next, c), at(z, x_prev, c)
    low_z, high_z = pl.ds(0, 4), pl.ds(4, 4)
    to_next = remote(kvb.at[c, x], kvb.at[c, x], x_send.at[0], x_recv.at[0], "ep", up_x)
    to_prev = remote(kvb.at[c, x], kvb.at[c, x], x_send.at[1], x_recv.at[1], "ep", down_x)
    on_next = remote(
        kvb.at[c, x_prev, low_z], kvb.at[c, x_prev, low_z], x_send.at[2], x_recv.at[2], "ep", up_x
    )
    on_prev = remote(
        kvb.at[c, x_next, high_z], kvb.at[c, x_next, high_z], x_send.at[3], x_recv.at[3], "ep", down_x
    )

    def to_core(block, n):
        return remote(
            kvb.at[c, block], kvb.at[c, block], core_send.at[n], core_recv.at[n],
            "ep", at(z, x, 1 - c),
        )

    blocks = (x, x_next, x_prev, x_far)

    local[0].wait()
    for i in range(1, N_Z):
        along_z(i).wait_recv()
    to_next.start()
    to_prev.start()
    to_core(blocks[0], 0).start()

    def dispatch(i, carry):
        peer = lax.rem(me + i, N_EP)
        remote(
            send_ref.at[peer], arrived.at[me], disp_send.at[0], disp_recv.at[0], "ep", peer
        ).start()
        return carry

    lax.fori_loop(1, N_EP, dispatch, 0)

    service(0)

    run_max[...] = jnp.full_like(run_max, -jnp.inf)
    run_sum[...] = jnp.zeros_like(run_sum)
    mixed[...] = jnp.zeros_like(mixed)

    def attention_step(t, carry):
        xi = lax.div(t, 2)
        x_rel = xi + lax.div(xi, 2) - 2 * lax.div(xi, 3)
        block = lax.rem(x + x_rel, N_X)
        core = lax.rem(c + lax.rem(t, 2), N_CORE)

        @pl.when(t == 1)
        def _():
            to_core(blocks[0], 0).wait_recv()

        @pl.when(t == 2)
        def _():
            to_prev.wait_recv()
            on_prev.start()
            to_core(x_next, 1).start()
            to_next.wait_recv()
            on_next.start()
            to_core(x_prev, 2).start()

        @pl.when(t == 3)
        def _():
            service(1)
            to_core(x_next, 1).wait_recv()

        @pl.when(t == 5)
        def _():
            to_core(x_prev, 2).wait_recv()

        @pl.when(t == 6)
        def _():
            on_next.wait_recv()
            on_prev.wait_recv()
            to_core(x_far, 3).start()

        @pl.when(t == 7)
        def _():
            service(2)
            to_core(x_far, 3).wait_recv()

        keys = kvb[core, block].reshape(N_Z * 256, 128)
        for qb in range(4):
            rows = slice(qb * 256, qb * 256 + 256)
            scores = lax.dot_general(q_ref[rows], keys, NT, preferred_element_type=F32)
            old = run_max[rows]
            new = jnp.maximum(old, jnp.max(scores, axis=1, keepdims=True))
            factor = jnp.exp(old - new)
            weights = jnp.exp(scores - new[:, :1])
            total = run_sum[rows] * factor
            for n in range(N_Z * 256 // 128):
                total = total + weights[:, n * 128 : n * 128 + 128]
            run_sum[rows] = total
            run_max[rows] = new
            mixed[rows] = mixed[rows] * factor + jnp.dot(
                weights.astype(BF16), keys, preferred_element_type=F32
            )
        return carry

    lax.fori_loop(0, 8, attention_step, 0)

    low = lax.broadcasted_iota(jnp.int32, (256, 128), 1) < 64
    for pair in range(2):
        base = pair * 512
        halves = []
        for h in range(2):
            rows = slice(base + h * 256, base + h * 256 + 256)
            halves.append(mixed[rows] / jnp.sum(run_sum[rows], axis=1, keepdims=True))
        attn_ref[:, pair * 128 : pair * 128 + 128] = jnp.where(
            low, pltpu.roll(halves[0], 64, 1), halves[1]
        ).astype(BF16)

    service(3)
    for copy in local[1:]:
        copy.wait()
    remote(
        send_ref.at[pl.ds(0, N_EP - 1)], arrived.at[pl.ds(0, N_EP - 1)],
        disp_send.at[0], disp_recv.at[0], "ep", up_x,
    ).wait()
    rows_bf[...] = arrived[...].astype(F32).reshape(N_EP * CAP, -1).astype(BF16)

    for slot in range(N_TP):
        if slot == 2:
            service(4)
        if slot == 3:
            for i in range(4):
                complete(i)
        rows_in = rows_bf[...]
        gate = jnp.dot(rows_in, wgb[slot], preferred_element_type=F32)
        up = jnp.dot(rows_in, wub[slot], preferred_element_type=F32)
        hidden[slot] = silu_times(gate, up)

    def send_back(j):
        def one(i, carry):
            peer = lax.rem(me + i, N_EP)
            remote(
                outbuf.at[j, peer], ret.at[j, me], ret_send.at[j], ret_recv.at[j], "ep", peer
            ).start()
            return carry

        lax.fori_loop(1, N_EP, one, 0)

    back = []
    for j in range(CHUNKS):
        service(5 + j)
        complete(4 + j)
        total = jnp.zeros((N_EP * CAP, 512), F32)
        for slot in range(N_TP):
            total = total + jnp.dot(
                hidden[slot], wdb[slot, j], preferred_element_type=F32
            ).astype(BF16).astype(F32)
        outbuf[j] = total.reshape(N_EP, CAP, 512).astype(BF16)
        send_back(j)
        copy = pltpu.make_async_copy(outbuf.at[j, me], ret.at[j, me], own_sem.at[12 + j])
        copy.start()
        back.append(copy)

    def shared_of(slot):
        rows_in = nall[slot]
        gate = jnp.dot(rows_in, sgb[...], preferred_element_type=F32)
        up = jnp.dot(rows_in, sub[...], preferred_element_type=F32)
        return jnp.dot(silu_times(gate, up), sdb[...], preferred_element_type=F32).astype(BF16)

    shares = {
        1: remote(part.at[1], parts.at[2], rs_send.at[1], rs_recv.at[2], "tp", left),
        2: remote(part.at[2], parts.at[1], rs_send.at[2], rs_recv.at[1], "tp", right),
        3: remote(part.at[3], parts.at[3], rs_send.at[3], rs_recv.at[3], "tp", opposite),
    }
    for slot in (1, 2):
        part[slot] = shared_of(slot)
        shares[slot].start()
    complete(8)
    part[3] = shared_of(3)
    shares[3].start()
    part[0] = shared_of(0)
    for slot in (1, 2, 3):
        shares[slot].wait_recv()

    for j in range(CHUNKS):
        columns = slice(j * 512, j * 512 + 512)
        back[j].wait()
        remote(
            outbuf.at[j, pl.ds(0, N_EP - 1)], ret.at[j, pl.ds(0, N_EP - 1)],
            ret_send.at[j], ret_recv.at[j], "ep", up_x,
        ).wait()
        flat = ret[j].astype(F32).reshape(N_EP * CAP, 512).astype(BF16)
        total = part[0, :, columns].astype(F32)
        for slot in (1, 2, 3):
            total = total + parts[slot, :, columns].astype(F32)
        for k in range(2):
            picked = jnp.dot(choose_ref[k], flat, preferred_element_type=F32)
            total = total + gates_ref[:, k : k + 1] * picked
        moe_ref[:, columns] = total.astype(BF16)

    for i in range(len(items)):
        for n in range(4):
            item_copy(i, n).wait_send()
    for i in range(1, N_Z):
        along_z(i).wait_send()
    for copy in (to_next, to_prev, on_next, on_prev):
        copy.wait_send()
    for n in range(4):
        to_core(blocks[n], n).wait_send()
    for slot in (1, 2, 3):
        shares[slot].wait_send()


def layer(q, kv, send, normed, choose, gates, wg, wu, wd, sg, su, sd):
    vmem = pl.BlockSpec(memory_space=pltpu.VMEM)
    anywhere = pl.BlockSpec(memory_space=pl.ANY)
    width = normed.shape[1]
    dma = pltpu.SemaphoreType.DMA
    return pl.pallas_call(
        layer_kernel,
        out_shape=[
            jax.ShapeDtypeStruct((256, 256), BF16),
            jax.ShapeDtypeStruct(normed.shape, BF16),
        ],
        in_specs=[vmem, anywhere, anywhere, anywhere, vmem, vmem] + [anywhere] * 6,
        out_specs=[vmem, vmem],
        scratch_shapes=[
            pltpu.VMEM((N_CORE, N_X, N_Z, 256, 128), BF16),
            pltpu.VMEM((1024, 128), F32),
            pltpu.VMEM((1024, 128), F32),
            pltpu.VMEM((1024, 128), F32),
            pltpu.VMEM((N_TP, width, 256), BF16),
            pltpu.VMEM((N_TP, width, 256), BF16),
            pltpu.VMEM((N_TP, CHUNKS, 256, 512), BF16),
            pltpu.VMEM((N_TP, 128, width), BF16),
            pltpu.VMEM((N_EP, CAP, width), BF16),
            pltpu.VMEM((N_EP * CAP, width), BF16),
            pltpu.VMEM((N_TP, N_EP * CAP, 256), BF16),
            pltpu.VMEM((CHUNKS, N_EP, CAP, 512), BF16),
            pltpu.VMEM((CHUNKS, N_EP, CAP, 512), BF16),
            pltpu.VMEM((width, 256), BF16),
            pltpu.VMEM((width, 256), BF16),
            pltpu.VMEM((256, width), BF16),
            pltpu.VMEM((N_TP, 128, width), BF16),
            pltpu.VMEM((N_TP, 128, width), BF16),
            dma((9, 4)), dma((9, 4)), dma((N_Z,)), dma((N_Z,)), dma((4,)), dma((4,)),
            dma((4,)), dma((4,)), dma((1,)), dma((1,)), dma((CHUNKS,)), dma((CHUNKS,)),
            dma((4,)), dma((4,)), dma((16,)),
        ],
        compiler_params=pltpu.CompilerParams(
            collective_id=1, has_side_effects=True, vmem_limit_bytes=60 * 1024 * 1024
        ),
        name="layer",
    )(q, kv, send, normed, choose, gates, wg, wu, wd, sg, su, sd)


def slot_numbers(own_routes, experts, capacity):
    tok_rows = own_routes.shape[0]
    named = own_routes[:, :, None] == jnp.arange(experts, dtype=jnp.int32)
    counts = jnp.any(named, axis=1).astype(BF16)
    rows = jnp.arange(tok_rows, dtype=jnp.int32)
    before = (rows[:, None] > rows[None, :]).astype(BF16)
    earlier = jnp.dot(before, counts, preferred_element_type=F32)
    ranks = jnp.sum(jnp.where(named, earlier[:, None, :], 0.0), axis=2).astype(jnp.int32)
    return own_routes * capacity + ranks


def body(
    query_rows, key_rows, value_rows, query_gain, key_gain, moe_tokens, norm_gain, routes,
    route_weights, expert_gate, expert_up, expert_down, shared_gate, shared_up, shared_down,
):
    tok_rows, model_width = moe_tokens.shape
    lane = lax.axis_index("tp")
    values32 = moe_tokens.astype(F32)
    normed = (
        values32
        * lax.rsqrt(jnp.mean(values32 * values32, axis=-1, keepdims=True) + epsilon)
        * norm_gain
    ).astype(BF16)
    own_routes = lax.dynamic_slice_in_dim(routes, lane * tok_rows, tok_rows, 0)
    own_weights = lax.dynamic_slice_in_dim(route_weights, lane * tok_rows, tok_rows, 0)
    own_gates = own_weights / jnp.sum(own_weights, axis=-1, keepdims=True) * routed_scale
    slots = slot_numbers(own_routes, N_EP, CAP)
    slot_ids = jnp.arange(N_EP * CAP, dtype=jnp.int32)
    placing = jnp.any(slot_ids[:, None, None] == slots[None, :, :], axis=2).astype(BF16)
    send = jnp.dot(placing, normed, preferred_element_type=F32).astype(BF16)
    send = send.reshape(N_EP, CAP, model_width)
    choose = (slots.T[:, :, None] == slot_ids[None, None, :]).astype(BF16)
    q, kv = prepared(query_rows, key_rows, value_rows, query_gain, key_gain)
    attn_out, moe_out = layer(
        q, kv, send, normed, choose, own_gates,
        expert_gate[0], expert_up[0], expert_down[0], shared_gate, shared_up, shared_down,
    )
    return attn_out, moe_out


def solution(mesh):
    return jax.shard_map(
        body,
        mesh=mesh,
        in_specs=(
            P("ep", "tp"), P("ep", "tp"), P("ep", "tp"), P(), P(),
            P(("ep", "tp"), None), P(), P("ep", None), P("ep", None),
            P("ep", None, "tp"), P("ep", None, "tp"), P("ep", "tp", None),
            P(None, "tp"), P(None, "tp"), P("tp", None),
        ),
        out_specs=(P("ep", "tp"), P(("ep", "tp"), None)),
        check_vma=False,
    )
```

```python
import functools

import jax
import jax.numpy as jnp
import numpy as np
from jax import lax
from jax.experimental import pallas as pl
from jax.experimental.pallas import tpu as pltpu
from jax.sharding import PartitionSpec as P

GRID_W = 64
TOKENS_A = 16384
MESH = pl.DeviceIdType.MESH
F32 = jnp.float32
BF16 = jnp.bfloat16

epsilon = 1e-06
rotary_base = 10000.0
routed_scale = 2.5

N_Z, N_X, N_CORE = 8, 4, 2
N_EP, N_TP = 64, 4
CAP = 8
CHUNKS = 4
NT = (((1,), (1,)), ((), ()))


def angle_tables():
    pairs = np.arange(128) % 64 // 2
    inv_freq = (rotary_base ** (-np.arange(16, dtype=np.float64) / 16)).astype(np.float32)
    freq = inv_freq[pairs % 16]
    sign = np.where(np.arange(128) % 2 == 0, -1.0, 1.0)
    tables = []
    for count, mask in ((TOKENS_A // GRID_W, pairs < 16), (GRID_W, pairs >= 16)):
        angles = (np.arange(count, dtype=np.float32)[:, None] * freq).astype(np.float64)
        tables.append((np.cos(angles) * mask).astype(np.float32))
        tables.append((np.sin(angles) * sign * mask).astype(np.float32))
    return tables


def silu_times(gate, up):
    return (gate / (1.0 + jnp.exp(-gate)) * up).astype(BF16)


def layer_kernel(
    query_ref, key_ref, value_ref, qgain_ref, kgain_ref, rcos_ref, rsin_ref, ccos_ref, csin_ref,
    tokens_ref, ngain_ref, routes_ref, scores_ref,
    wg_ref, wu_ref, wd_ref, sg_ref, su_ref, sd_ref,
    attn_ref, moe_ref,
    q_ref, normed_ref, send_ref, choose_ref, gates_ref,
    kvb, run_max, run_sum, mixed,
    wgb, wub, wdb, nall, arrived, rows_bf, hidden, outbuf, ret,
    sgb, sub, sdb, part, parts,
    item_send, item_recv, kv_send, kv_recv, x_send, x_recv, core_send, core_recv,
    disp_send, disp_recv, ret_send, ret_recv, rs_send, rs_recv, own_sem,
):
    me, lane = lax.axis_index("ep"), lax.axis_index("tp")
    z, x, c = lax.div(me, 8), lax.rem(lax.div(me, 2), 4), lax.rem(me, 2)
    right, left = lax.rem(lane + 1, N_TP), lax.rem(lane + 3, N_TP)
    opposite = lax.rem(lane + 2, N_TP)

    def at(zz, xx, cc):
        return (zz * N_X + xx) * N_CORE + cc

    def remote(src, dst, send_sem, recv_sem, axis, peer):
        return pltpu.make_async_remote_copy(
            src_ref=src, dst_ref=dst, send_sem=send_sem, recv_sem=recv_sem,
            device_id={axis: peer}, device_id_type=MESH,
        )

    barrier = pltpu.get_barrier_semaphore()

    def greet(i, carry):
        pl.semaphore_signal(
            barrier, inc=1, device_id={"ep": lax.rem(me + i, N_EP)}, device_id_type=MESH
        )
        return carry

    for i in range(1, N_TP):
        pl.semaphore_signal(
            barrier, inc=1, device_id={"tp": lax.rem(lane + i, N_TP)}, device_id_type=MESH
        )
    lax.fori_loop(1, N_EP, greet, 0)
    pl.semaphore_wait(barrier, N_EP - 1 + N_TP - 1)

    items = []
    for ref, buf in ((wg_ref, wgb), (wu_ref, wub)):
        for h in range(2):
            items.append((ref.at[pl.ds(h * 1024, 1024)], buf, (pl.ds(h * 1024, 1024),), h * 1024, 512))
    for j in range(CHUNKS):
        items.append((wd_ref.at[:, pl.ds(j * 512, 512)], wdb, (j,), 0, 128))
    items.append((normed_ref, nall, (), 0, 64))

    def item_copy(i, n):
        src, buf, where, base, half = items[i]
        lead = where[:-1] if where and not isinstance(where[0], int) else where
        s, r = item_send.at[i], item_recv.at[i]
        lower, upper = pl.ds(base, half), pl.ds(base + half, half)

        def piece(slot, rows):
            return buf.at[(slot,) + lead + (rows,)]

        if n == 0:
            return remote(src, buf.at[(1,) + where], s.at[0], r.at[0], "tp", right)
        if n == 1:
            return remote(src, buf.at[(2,) + where], s.at[1], r.at[1], "tp", left)
        if n == 2:
            return remote(piece(1, lower), piece(3, lower), s.at[2], r.at[2], "tp", right)
        return remote(piece(2, upper), piece(3, upper), s.at[3], r.at[3], "tp", left)

    def begin(i):
        if i < len(items):
            item_copy(i, 0).start()
            item_copy(i, 1).start()

    def service(i):
        item_copy(i, 0).wait_recv()
        item_copy(i, 2).start()
        item_copy(i, 1).wait_recv()
        item_copy(i, 3).start()
        begin(i + 3)

    def complete(i):
        item_copy(i, 2).wait_recv()
        item_copy(i, 3).wait_recv()

    begin(0)
    begin(1)
    begin(2)

    rows = query_ref.shape[0]
    lanes = lax.broadcasted_iota(jnp.int32, (rows, 128), 1)
    low, even = lanes < 64, lax.rem(lanes, 2) == 0
    grid_rows = rows // GRID_W

    def table(row_ref, col_ref):
        return jnp.concatenate(
            [row_ref[pl.ds(me * grid_rows + n, 1), :] + col_ref[...] for n in range(grid_rows)], axis=0
        )

    cosine, sine = table(rcos_ref, ccos_ref), table(rsin_ref, csin_ref)

    def turned(values, gain):
        squares = values * values
        first = jnp.sum(jnp.where(low, squares, 0.0), axis=1, keepdims=True) / 64.0
        second = jnp.sum(jnp.where(low, 0.0, squares), axis=1, keepdims=True) / 64.0
        inverse = jnp.where(low, lax.rsqrt(first + epsilon), lax.rsqrt(second + epsilon))
        y = values * inverse * gain
        partner = jnp.where(even, pltpu.roll(y, 127, 1), pltpu.roll(y, 1, 1))
        return (y * cosine + partner * sine).astype(BF16).astype(F32)

    def both(gain_ref):
        return jnp.concatenate([gain_ref[...], gain_ref[...]], axis=1)

    kv = jnp.concatenate([key_ref[...].astype(F32), value_ref[...].astype(F32)], axis=0).T
    kvb[c, x, z] = jnp.where(low, turned(kv, both(kgain_ref)), kv).astype(BF16)

    def along_z(i):
        return remote(
            kvb.at[c, x, z], kvb.at[c, x, z], kv_send.at[i], kv_recv.at[i],
            "ep", at(lax.rem(z + i, N_Z), x, c),
        )

    for i in range(1, N_Z):
        along_z(i).start()

    local = []
    for n, (src, dst) in enumerate((
        (wg_ref, wgb.at[0]), (wu_ref, wub.at[0]), (sg_ref, sgb), (su_ref, sub), (sd_ref, sdb),
    )):
        local.append(pltpu.make_async_copy(src, dst, own_sem.at[n]))
    for j in range(CHUNKS):
        local.append(pltpu.make_async_copy(
            wd_ref.at[:, pl.ds(j * 512, 512)], wdb.at[0, j], own_sem.at[8 + j]
        ))
    for copy in local:
        copy.start()

    gain = both(qgain_ref)
    for pair in range(2):
        values = query_ref[:, pair * 128 : pair * 128 + 128].astype(F32)
        out = turned(values, gain) * 0.125
        base = 2 * pair * rows
        q_ref[base : base + rows, :] = jnp.where(low, out, 0.0).astype(BF16)
        q_ref[base + rows : base + 2 * rows, :] = jnp.where(
            low, pltpu.roll(out, 64, 1), 0.0
        ).astype(BF16)

    values = tokens_ref[...].astype(F32)
    normed_ref[...] = (
        values
        * lax.rsqrt(jnp.mean(values * values, axis=-1, keepdims=True) + epsilon)
        * ngain_ref[...]
    ).astype(BF16)
    own_rows = pl.ds(pl.multiple_of(lane * 128, 128), 128)
    routes = routes_ref[:, own_rows]
    expert_ids = lax.broadcasted_iota(jnp.int32, (N_EP, 128), 0)
    named = [expert_ids == routes[k : k + 1, :] for k in range(2)]
    counts = jnp.where(named[0] | named[1], 1.0, 0.0).astype(BF16)
    square = (128, 128)
    before = jnp.where(
        lax.broadcasted_iota(jnp.int32, square, 0) < lax.broadcasted_iota(jnp.int32, square, 1), 1.0, 0.0
    ).astype(BF16)
    earlier = jnp.dot(counts, before, preferred_element_type=F32)
    slot_ids = lax.broadcasted_iota(jnp.int32, (N_EP * CAP, 128), 0).astype(F32)
    placing = 0.0
    for k in range(2):
        rank = jnp.sum(jnp.where(named[k], earlier, 0.0), axis=0, keepdims=True)
        place = jnp.where(slot_ids == routes[k : k + 1, :].astype(F32) * CAP + rank, 1.0, 0.0)
        placing = placing + place
        choose_ref[k] = place.T.astype(BF16)
    send_ref[...] = jnp.dot(
        placing.astype(BF16), normed_ref[...], preferred_element_type=F32
    ).reshape(N_EP, CAP, -1).astype(BF16)
    scores = scores_ref[:, own_rows]
    gates = scores / (scores[0:1] + scores[1:2]) * routed_scale
    for k in range(2):
        gates_ref[k] = jnp.broadcast_to(gates[k : k + 1], square).T
    arrived[me] = send_ref[me]
    nall[0] = normed_ref[...]

    x_next, x_prev = lax.rem(x + 1, N_X), lax.rem(x + 3, N_X)
    x_far = lax.rem(x + 2, N_X)
    up_x, down_x = at(z, x_next, c), at(z, x_prev, c)
    low_z, high_z = pl.ds(0, 4), pl.ds(4, 4)
    to_next = remote(kvb.at[c, x], kvb.at[c, x], x_send.at[0], x_recv.at[0], "ep", up_x)
    to_prev = remote(kvb.at[c, x], kvb.at[c, x], x_send.at[1], x_recv.at[1], "ep", down_x)
    on_next = remote(
        kvb.at[c, x_prev, low_z], kvb.at[c, x_prev, low_z], x_send.at[2], x_recv.at[2], "ep", up_x
    )
    on_prev = remote(
        kvb.at[c, x_next, high_z], kvb.at[c, x_next, high_z], x_send.at[3], x_recv.at[3], "ep", down_x
    )

    def to_core(block, n):
        return remote(
            kvb.at[c, block], kvb.at[c, block], core_send.at[n], core_recv.at[n],
            "ep", at(z, x, 1 - c),
        )

    blocks = (x, x_next, x_prev, x_far)

    for i in range(1, N_Z):
        along_z(i).wait_recv()
    to_next.start()
    to_prev.start()
    to_core(blocks[0], 0).start()

    def dispatch(i, carry):
        peer = lax.rem(me + i, N_EP)
        remote(
            send_ref.at[peer], arrived.at[me], disp_send.at[0], disp_recv.at[0], "ep", peer
        ).start()
        return carry

    lax.fori_loop(1, N_EP, dispatch, 0)

    service(0)

    run_max[...] = jnp.full_like(run_max, -jnp.inf)
    run_sum[...] = jnp.zeros_like(run_sum)
    mixed[...] = jnp.zeros_like(mixed)

    def attention_step(t, carry):
        xi = lax.div(t, 2)
        x_rel = xi + lax.div(xi, 2) - 2 * lax.div(xi, 3)
        block = lax.rem(x + x_rel, N_X)
        core = lax.rem(c + lax.rem(t, 2), N_CORE)

        @pl.when(t == 1)
        def _():
            to_core(blocks[0], 0).wait_recv()

        @pl.when(t == 2)
        def _():
            service(1)
            to_prev.wait_recv()
            on_prev.start()
            to_core(x_next, 1).start()
            to_next.wait_recv()
            on_next.start()
            to_core(x_prev, 2).start()

        @pl.when(t == 3)
        def _():
            to_core(x_next, 1).wait_recv()

        @pl.when(t == 4)
        def _():
            service(2)

        @pl.when(t == 5)
        def _():
            to_core(x_prev, 2).wait_recv()

        @pl.when(t == 6)
        def _():
            service(3)
            on_next.wait_recv()
            on_prev.wait_recv()
            to_core(x_far, 3).start()

        @pl.when(t == 7)
        def _():
            to_core(x_far, 3).wait_recv()

        keys = kvb[core, block].reshape(N_Z * 256, 128)
        for qb in range(4):
            rows = slice(qb * 256, qb * 256 + 256)
            scores = lax.dot_general(q_ref[rows], keys, NT, preferred_element_type=F32)
            old = run_max[rows]
            new = jnp.maximum(old, jnp.max(scores, axis=1, keepdims=True))
            factor = jnp.exp(old - new)
            weights = jnp.exp(scores - new[:, :1])
            total = run_sum[rows] * factor
            for n in range(N_Z * 256 // 128):
                total = total + weights[:, n * 128 : n * 128 + 128]
            run_sum[rows] = total
            run_max[rows] = new
            mixed[rows] = mixed[rows] * factor + jnp.dot(
                weights.astype(BF16), keys, preferred_element_type=F32
            )
        return carry

    lax.fori_loop(0, 8, attention_step, 0)

    for pair in range(2):
        base = pair * 512
        halves = []
        for h in range(2):
            rows = slice(base + h * 256, base + h * 256 + 256)
            halves.append(mixed[rows] / jnp.sum(run_sum[rows], axis=1, keepdims=True))
        attn_ref[:, pair * 128 : pair * 128 + 128] = jnp.where(
            low, pltpu.roll(halves[0], 64, 1), halves[1]
        ).astype(BF16)

    service(4)
    for copy in local:
        copy.wait()
    remote(
        send_ref.at[pl.ds(0, N_EP - 1)], arrived.at[pl.ds(0, N_EP - 1)],
        disp_send.at[0], disp_recv.at[0], "ep", up_x,
    ).wait()
    rows_bf[...] = arrived[...].astype(F32).reshape(N_EP * CAP, -1).astype(BF16)

    for slot in range(N_TP):
        if slot == 2:
            service(5)
        if slot == 3:
            for i in range(4):
                complete(i)
        rows_in = rows_bf[...]
        gate = jnp.dot(rows_in, wgb[slot], preferred_element_type=F32)
        up = jnp.dot(rows_in, wub[slot], preferred_element_type=F32)
        hidden[slot] = silu_times(gate, up)

    def send_back(j):
        def one(i, carry):
            peer = lax.rem(me + i, N_EP)
            remote(
                outbuf.at[j, peer], ret.at[j, me], ret_send.at[j], ret_recv.at[j], "ep", peer
            ).start()
            return carry

        lax.fori_loop(1, N_EP, one, 0)

    back = []
    for j in range(CHUNKS):
        if j < 3:
            service(6 + j)
        complete(4 + j)
        total = jnp.zeros((N_EP * CAP, 512), F32)
        for slot in range(N_TP):
            total = total + jnp.dot(
                hidden[slot], wdb[slot, j], preferred_element_type=F32
            ).astype(BF16).astype(F32)
        outbuf[j] = total.reshape(N_EP, CAP, 512).astype(BF16)
        send_back(j)
        copy = pltpu.make_async_copy(outbuf.at[j, me], ret.at[j, me], own_sem.at[12 + j])
        copy.start()
        back.append(copy)

    def shared_of(slot):
        rows_in = nall[slot]
        gate = jnp.dot(rows_in, sgb[...], preferred_element_type=F32)
        up = jnp.dot(rows_in, sub[...], preferred_element_type=F32)
        return jnp.dot(silu_times(gate, up), sdb[...], preferred_element_type=F32).astype(BF16)

    shares = {
        1: remote(part.at[1], parts.at[2], rs_send.at[1], rs_recv.at[2], "tp", left),
        2: remote(part.at[2], parts.at[1], rs_send.at[2], rs_recv.at[1], "tp", right),
        3: remote(part.at[3], parts.at[3], rs_send.at[3], rs_recv.at[3], "tp", opposite),
    }
    for slot in (1, 2):
        part[slot] = shared_of(slot)
        shares[slot].start()
    complete(8)
    part[3] = shared_of(3)
    shares[3].start()
    part[0] = shared_of(0)
    for slot in (1, 2, 3):
        shares[slot].wait_recv()

    for j in range(CHUNKS):
        columns = slice(j * 512, j * 512 + 512)
        back[j].wait()
        remote(
            outbuf.at[j, pl.ds(0, N_EP - 1)], ret.at[j, pl.ds(0, N_EP - 1)],
            ret_send.at[j], ret_recv.at[j], "ep", up_x,
        ).wait()
        flat = ret[j].astype(F32).reshape(N_EP * CAP, 512).astype(BF16)
        total = part[0, :, columns].astype(F32)
        for slot in (1, 2, 3):
            total = total + parts[slot, :, columns].astype(F32)
        for k in range(2):
            picked = jnp.dot(choose_ref[k], flat, preferred_element_type=F32)
            total = total + gates_ref[k, :, 0:1] * picked
        moe_ref[:, columns] = total.astype(BF16)

    for i in range(len(items)):
        for n in range(4):
            item_copy(i, n).wait_send()
    for i in range(1, N_Z):
        along_z(i).wait_send()
    for copy in (to_next, to_prev, on_next, on_prev):
        copy.wait_send()
    for n in range(4):
        to_core(blocks[n], n).wait_send()
    for slot in (1, 2, 3):
        shares[slot].wait_send()


def layer(tokens, small, weights):
    vmem = pl.BlockSpec(memory_space=pltpu.VMEM)
    anywhere = pl.BlockSpec(memory_space=pl.ANY)
    width = tokens.shape[1]
    dma = pltpu.SemaphoreType.DMA
    return pl.pallas_call(
        layer_kernel,
        out_shape=[
            jax.ShapeDtypeStruct((256, 256), BF16),
            jax.ShapeDtypeStruct(tokens.shape, BF16),
        ],
        in_specs=[vmem] * len(small) + [anywhere] * len(weights),
        out_specs=[vmem, vmem],
        scratch_shapes=[
            pltpu.VMEM((1024, 128), BF16),
            pltpu.VMEM((128, width), BF16),
            pltpu.VMEM((N_EP, CAP, width), BF16),
            pltpu.VMEM((2, 128, N_EP * CAP), BF16),
            pltpu.VMEM((2, 128, 128), F32),
            pltpu.VMEM((N_CORE, N_X, N_Z, 256, 128), BF16),
            pltpu.VMEM((1024, 128), F32),
            pltpu.VMEM((1024, 128), F32),
            pltpu.VMEM((1024, 128), F32),
            pltpu.VMEM((N_TP, width, 256), BF16),
            pltpu.VMEM((N_TP, width, 256), BF16),
            pltpu.VMEM((N_TP, CHUNKS, 256, 512), BF16),
            pltpu.VMEM((N_TP, 128, width), BF16),
            pltpu.VMEM((N_EP, CAP, width), BF16),
            pltpu.VMEM((N_EP * CAP, width), BF16),
            pltpu.VMEM((N_TP, N_EP * CAP, 256), BF16),
            pltpu.VMEM((CHUNKS, N_EP, CAP, 512), BF16),
            pltpu.VMEM((CHUNKS, N_EP, CAP, 512), BF16),
            pltpu.VMEM((width, 256), BF16),
            pltpu.VMEM((width, 256), BF16),
            pltpu.VMEM((256, width), BF16),
            pltpu.VMEM((N_TP, 128, width), BF16),
            pltpu.VMEM((N_TP, 128, width), BF16),
            dma((9, 4)), dma((9, 4)), dma((N_Z,)), dma((N_Z,)), dma((4,)), dma((4,)),
            dma((4,)), dma((4,)), dma((1,)), dma((1,)), dma((CHUNKS,)), dma((CHUNKS,)),
            dma((4,)), dma((4,)), dma((16,)),
        ],
        compiler_params=pltpu.CompilerParams(
            collective_id=1, has_side_effects=True, vmem_limit_bytes=60 * 1024 * 1024
        ),
        name="layer",
    )(*small, *weights)


def body(
    query_rows, key_rows, value_rows, query_gain, key_gain, moe_tokens, norm_gain, routes,
    route_weights, expert_gate, expert_up, expert_down, shared_gate, shared_up, shared_down,
):
    small = (
        query_rows, key_rows.T, value_rows.T, query_gain[None, :], key_gain[None, :],
        *(jnp.asarray(table) for table in angle_tables()),
        moe_tokens, norm_gain[None, :], routes.T, route_weights.T,
    )
    weights = (
        expert_gate[0], expert_up[0], expert_down[0], shared_gate, shared_up, shared_down,
    )
    return tuple(layer(moe_tokens, small, weights))


def solution(mesh):
    return jax.shard_map(
        body,
        mesh=mesh,
        in_specs=(
            P("ep", "tp"), P("ep", "tp"), P("ep", "tp"), P(), P(),
            P(("ep", "tp"), None), P(), P("ep", None), P("ep", None),
            P("ep", None, "tp"), P("ep", None, "tp"), P("ep", "tp", None),
            P(None, "tp"), P(None, "tp"), P("tp", None),
        ),
        out_specs=(P("ep", "tp"), P(("ep", "tp"), None)),
        check_vma=False,
    )
```

```python
import functools

import jax
import jax.numpy as jnp
import numpy as np
from jax import lax
from jax.experimental import pallas as pl
from jax.experimental.pallas import tpu as pltpu
from jax.sharding import PartitionSpec as P

GRID_W = 64
TOKENS_A = 16384
MESH = pl.DeviceIdType.MESH
F32 = jnp.float32
BF16 = jnp.bfloat16

epsilon = 1e-06
rotary_base = 10000.0
routed_scale = 2.5

N_Z, N_X, N_CORE = 8, 4, 2
N_EP, N_TP = 64, 4
CAP = 8
CHUNKS = ((0, 256), (256, 256), (512, 512), (1024, 512), (1536, 512))
NT = (((1,), (1,)), ((), ()))


def angle_tables():
    pairs = np.arange(128) % 64 // 2
    inv_freq = (rotary_base ** (-np.arange(16, dtype=np.float64) / 16)).astype(np.float32)
    freq = inv_freq[pairs % 16]
    sign = np.where(np.arange(128) % 2 == 0, -1.0, 1.0)
    tables = []
    for count, mask in ((TOKENS_A // GRID_W, pairs < 16), (GRID_W, pairs >= 16)):
        angles = (np.arange(count, dtype=np.float32)[:, None] * freq).astype(np.float64)
        tables.append((np.cos(angles) * mask).astype(np.float32))
        tables.append((np.sin(angles) * sign * mask).astype(np.float32))
    return tables


def silu_times(gate, up):
    return (gate / (1.0 + jnp.exp(-gate)) * up).astype(BF16)


def layer_kernel(
    query_ref, key_ref, value_ref, qgain_ref, kgain_ref, rcos_ref, rsin_ref, ccos_ref, csin_ref,
    tokens_ref, ngain_ref, routes_ref, scores_ref,
    wg_ref, wu_ref, wd_ref, sg_ref, su_ref, sd_ref,
    attn_out, moe_out,
    attn_ref, moe_ref, q_ref, normed_ref, send_ref, choose_ref, gates_ref,
    kvb, run_max, run_sum, mixed,
    wgb, wub, wdb, arrived, rows_bf, hidden, outbuf, ret,
    sgb, sub, sdb, shared,
    item_send, item_recv, kv_send, kv_recv, x_send, x_recv, core_send, core_recv,
    disp_send, disp_recv, ret_send, ret_recv, unit_send, unit_recv, ring_send, ring_recv,
    wide_send, wide_recv, pair_send, pair_recv, own_sem,
):
    me, lane = lax.axis_index("ep"), lax.axis_index("tp")
    z, x, c = lax.div(me, 8), lax.rem(lax.div(me, 2), 4), lax.rem(me, 2)
    right, left = lax.rem(lane + 1, N_TP), lax.rem(lane + 3, N_TP)
    opposite = lax.rem(lane + 2, N_TP)

    def at(zz, xx, cc):
        return (zz * N_X + xx) * N_CORE + cc

    def remote(src, dst, send_sem, recv_sem, axis, peer):
        return pltpu.make_async_remote_copy(
            src_ref=src, dst_ref=dst, send_sem=send_sem, recv_sem=recv_sem,
            device_id={axis: peer}, device_id_type=MESH,
        )

    barrier = pltpu.get_barrier_semaphore()

    def greet(i, carry):
        pl.semaphore_signal(
            barrier, inc=1, device_id={"ep": lax.rem(me + i, N_EP)}, device_id_type=MESH
        )
        return carry

    for i in range(1, N_TP):
        pl.semaphore_signal(
            barrier, inc=1, device_id={"tp": lax.rem(lane + i, N_TP)}, device_id_type=MESH
        )
    lax.fori_loop(1, N_EP, greet, 0)
    pl.semaphore_wait(barrier, N_EP - 1 + N_TP - 1)

    items = []
    for ref, buf in ((wg_ref, wgb), (wu_ref, wub)):
        for h in range(2):
            items.append((ref.at[pl.ds(h * 1024, 1024)], buf, (pl.ds(h * 1024, 1024),), h * 1024, 512))
    for first, count in CHUNKS:
        items.append((wd_ref.at[:, pl.ds(first, count)], wdb, (slice(None), pl.ds(first, count)), 0, 128))

    def item_copy(i, n):
        src, buf, where, base, half = items[i]
        s, r = item_send.at[i], item_recv.at[i]
        lower, upper = pl.ds(base, half), pl.ds(base + half, half)

        def piece(slot, rows):
            return buf.at[(slot, rows) + where[1:]]

        if n == 0:
            return remote(src, buf.at[(1,) + where], s.at[0], r.at[0], "tp", right)
        if n == 1:
            return remote(src, buf.at[(2,) + where], s.at[1], r.at[1], "tp", left)
        if n == 2:
            return remote(piece(1, lower), piece(3, lower), s.at[2], r.at[2], "tp", right)
        return remote(piece(2, upper), piece(3, upper), s.at[3], r.at[3], "tp", left)

    def begin(i):
        item_copy(i, 0).start()
        item_copy(i, 1).start()

    def service(i):
        item_copy(i, 0).wait_recv()
        item_copy(i, 2).start()
        item_copy(i, 1).wait_recv()
        item_copy(i, 3).start()
        for later in follows.get(i, ()):
            begin(later)

    follows = {0: (3,), 3: (4, 5), 4: (6,), 5: (7,), 6: (8,)}

    def complete(i):
        item_copy(i, 2).wait_recv()
        item_copy(i, 3).wait_recv()

    column = pl.ds(pl.multiple_of(((c * N_X + x) * 2 + lax.div(z, 4)) * 128, 128), 128)
    bufs = (sgb, sub, sdb)
    shares = (sg_ref.at[c, x, z], su_ref.at[c, x, z], sd_ref.at[lax.rem(z, 4), :, column])
    others = pl.ds(1, N_TP - 1)

    def unit_copy(b, slot):
        peer = {1: right, 2: left, 3: opposite}[slot]
        return remote(
            shares[b], bufs[b].at[slot, c, x, z], unit_send.at[b, slot], unit_recv.at[b, slot], "tp", peer
        )

    def ring_copy(b, step, up):
        origin = lax.rem(z + (N_Z - step + 1 if up else step - 1), N_Z)
        ref = bufs[b].at[others, c, x, origin]
        n = step - 1 if up else step + 3
        to = lax.rem(z + (1 if up else N_Z - 1), N_Z)
        return remote(ref, ref, ring_send.at[b, n], ring_recv.at[b, n], "ep", at(to, x, c))

    ring_steps = ((1, True), (1, False), (2, True), (2, False), (3, True), (3, False), (4, True))

    def ring_begin(step):
        for b in range(3):
            ring_copy(b, step, True).start()
            if step < 4:
                ring_copy(b, step, False).start()

    def ring_finish(step):
        for b in range(3):
            ring_copy(b, step, True).wait_recv()
            if step < 4:
                ring_copy(b, step, False).wait_recv()

    for slot in range(1, N_TP):
        for b in range(3):
            unit_copy(b, slot).start()
    begin(0)
    begin(1)
    begin(2)

    rows = query_ref.shape[0]
    lanes = lax.broadcasted_iota(jnp.int32, (rows, 128), 1)
    low, even = lanes < 64, lax.rem(lanes, 2) == 0
    grid_rows = rows // GRID_W

    def table(row_ref, col_ref):
        return jnp.concatenate(
            [row_ref[pl.ds(me * grid_rows + n, 1), :] + col_ref[...] for n in range(grid_rows)], axis=0
        )

    cosine, sine = table(rcos_ref, ccos_ref), table(rsin_ref, csin_ref)

    def turned(values, gain):
        squares = values * values
        first = jnp.sum(jnp.where(low, squares, 0.0), axis=1, keepdims=True) / 64.0
        second = jnp.sum(jnp.where(low, 0.0, squares), axis=1, keepdims=True) / 64.0
        inverse = jnp.where(low, lax.rsqrt(first + epsilon), lax.rsqrt(second + epsilon))
        y = values * inverse * gain
        partner = jnp.where(even, pltpu.roll(y, 127, 1), pltpu.roll(y, 1, 1))
        return (y * cosine + partner * sine).astype(BF16).astype(F32)

    def both(gain_ref):
        return jnp.concatenate([gain_ref[...], gain_ref[...]], axis=1)

    kv = jnp.concatenate([key_ref[...].astype(F32), value_ref[...].astype(F32)], axis=0).T
    kvb[c, x, z] = jnp.where(low, turned(kv, both(kgain_ref)), kv).astype(BF16)

    def along_z(i):
        return remote(
            kvb.at[c, x, z], kvb.at[c, x, z], kv_send.at[i], kv_recv.at[i],
            "ep", at(lax.rem(z + i, N_Z), x, c),
        )

    for i in range(1, N_Z):
        along_z(i).start()

    local = []
    for n, (src, dst) in enumerate((
        (wg_ref, wgb.at[0]), (wu_ref, wub.at[0]), (sg_ref, sgb.at[0]), (su_ref, sub.at[0]),
    )):
        local.append(pltpu.make_async_copy(src, dst, own_sem.at[n]))
    local.append(pltpu.make_async_copy(wd_ref, wdb.at[0], own_sem.at[4]))
    for n in range(16):
        local.append(pltpu.make_async_copy(
            sd_ref.at[:, :, pl.ds(n * 128, 128)],
            sdb.at[0, n // 8, n // 2 % 4, pl.ds(n % 2 * 4, 4)], own_sem.at[16 + n],
        ))
    for copy in local:
        copy.start()
    for slot in range(1, N_TP):
        for b in range(3):
            unit_copy(b, slot).wait_recv()
    ring_begin(1)

    gain = both(qgain_ref)
    for pair in range(2):
        values = query_ref[:, pair * 128 : pair * 128 + 128].astype(F32)
        out = turned(values, gain) * 0.125
        base = 2 * pair * rows
        q_ref[base : base + rows, :] = jnp.where(low, out, 0.0).astype(BF16)
        q_ref[base + rows : base + 2 * rows, :] = jnp.where(
            low, pltpu.roll(out, 64, 1), 0.0
        ).astype(BF16)

    values = tokens_ref[...].astype(F32)
    normed_ref[...] = (
        values
        * lax.rsqrt(jnp.mean(values * values, axis=-1, keepdims=True) + epsilon)
        * ngain_ref[...]
    ).astype(BF16)
    own_rows = pl.ds(pl.multiple_of(lane * 128, 128), 128)
    routes = routes_ref[:, own_rows]
    expert_ids = lax.broadcasted_iota(jnp.int32, (N_EP, 128), 0)
    named = [expert_ids == routes[k : k + 1, :] for k in range(2)]
    counts = jnp.where(named[0] | named[1], 1.0, 0.0).astype(BF16)
    square = (128, 128)
    before = jnp.where(
        lax.broadcasted_iota(jnp.int32, square, 0) < lax.broadcasted_iota(jnp.int32, square, 1), 1.0, 0.0
    ).astype(BF16)
    earlier = jnp.dot(counts, before, preferred_element_type=F32)
    slot_ids = lax.broadcasted_iota(jnp.int32, (N_EP * CAP, 128), 0).astype(F32)
    placing = 0.0
    for k in range(2):
        rank = jnp.sum(jnp.where(named[k], earlier, 0.0), axis=0, keepdims=True)
        place = jnp.where(slot_ids == routes[k : k + 1, :].astype(F32) * CAP + rank, 1.0, 0.0)
        placing = placing + place
        choose_ref[k] = place.T.astype(BF16)
    send_ref[...] = jnp.dot(
        placing.astype(BF16), normed_ref[...], preferred_element_type=F32
    ).reshape(N_EP, CAP, -1).astype(BF16)
    scores = scores_ref[:, own_rows]
    gates = scores / (scores[0:1] + scores[1:2]) * routed_scale
    for k in range(2):
        gates_ref[k] = jnp.broadcast_to(gates[k : k + 1], square).T
    arrived[me] = send_ref[me]
    ring_finish(1)
    ring_begin(2)

    x_next, x_prev = lax.rem(x + 1, N_X), lax.rem(x + 3, N_X)
    x_far = lax.rem(x + 2, N_X)
    up_x, down_x = at(z, x_next, c), at(z, x_prev, c)
    low_z, high_z = pl.ds(0, 4), pl.ds(4, 4)
    to_next = remote(kvb.at[c, x], kvb.at[c, x], x_send.at[0], x_recv.at[0], "ep", up_x)
    to_prev = remote(kvb.at[c, x], kvb.at[c, x], x_send.at[1], x_recv.at[1], "ep", down_x)
    on_next = remote(
        kvb.at[c, x_prev, low_z], kvb.at[c, x_prev, low_z], x_send.at[2], x_recv.at[2], "ep", up_x
    )
    on_prev = remote(
        kvb.at[c, x_next, high_z], kvb.at[c, x_next, high_z], x_send.at[3], x_recv.at[3], "ep", down_x
    )

    def to_core(block, n):
        return remote(
            kvb.at[c, block], kvb.at[c, block], core_send.at[n], core_recv.at[n],
            "ep", at(z, x, 1 - c),
        )

    blocks = (x, x_next, x_prev, x_far)

    for i in range(1, N_Z):
        along_z(i).wait_recv()
    to_next.start()
    to_prev.start()
    to_core(blocks[0], 0).start()

    ring_finish(2)
    ring_begin(3)

    def wide_copy(b, n):
        if n < 2:
            ref = bufs[b].at[others, c, x]
        elif n == 2:
            ref = bufs[b].at[others, c, x_prev, low_z]
        else:
            ref = bufs[b].at[others, c, x_next, high_z]
        return remote(ref, ref, wide_send.at[b, n], wide_recv.at[b, n], "ep", (up_x, down_x)[n % 2])

    def pair_copy(b, n):
        ref = bufs[b].at[others, c, blocks[n]]
        return remote(ref, ref, pair_send.at[b, n], pair_recv.at[b, n], "ep", at(z, x, 1 - c))

    ring_finish(3)
    ring_begin(4)

    def dispatch(i, carry):
        peer = lax.rem(me + i, N_EP)
        remote(
            send_ref.at[peer], arrived.at[me], disp_send.at[0], disp_recv.at[0], "ep", peer
        ).start()
        return carry

    lax.fori_loop(1, N_EP, dispatch, 0)

    service(0)

    run_max[...] = jnp.full_like(run_max, -jnp.inf)
    run_sum[...] = jnp.zeros_like(run_sum)
    mixed[...] = jnp.zeros_like(mixed)

    def attention_step(t, carry):
        xi = lax.div(t, 2)
        x_rel = xi + lax.div(xi, 2) - 2 * lax.div(xi, 3)
        block = lax.rem(x + x_rel, N_X)
        core = lax.rem(c + lax.rem(t, 2), N_CORE)

        @pl.when(t == 1)
        def _():
            to_core(blocks[0], 0).wait_recv()

        @pl.when(t == 2)
        def _():
            service(1)
            to_prev.wait_recv()
            on_prev.start()
            to_core(x_next, 1).start()
            to_next.wait_recv()
            on_next.start()
            to_core(x_prev, 2).start()

        @pl.when(t == 3)
        def _():
            to_core(x_next, 1).wait_recv()
            ring_finish(4)
            for b in range(3):
                wide_copy(b, 0).start()
                wide_copy(b, 1).start()
                pair_copy(b, 0).start()

        @pl.when(t == 4)
        def _():
            service(2)

        @pl.when(t == 5)
        def _():
            to_core(x_prev, 2).wait_recv()

        @pl.when(t == 6)
        def _():
            service(3)
            on_next.wait_recv()
            on_prev.wait_recv()
            to_core(x_far, 3).start()

        @pl.when(t == 7)
        def _():
            to_core(x_far, 3).wait_recv()

        keys = kvb[core, block].reshape(N_Z * 256, 128)
        for qb in range(4):
            rows = slice(qb * 256, qb * 256 + 256)
            scores = lax.dot_general(q_ref[rows], keys, NT, preferred_element_type=F32)
            old = run_max[rows]
            new = jnp.maximum(old, jnp.max(scores, axis=1, keepdims=True))
            factor = jnp.exp(old - new)
            weights = jnp.exp(scores - new[:, :1])
            total = run_sum[rows] * factor
            for n in range(N_Z * 256 // 128):
                total = total + weights[:, n * 128 : n * 128 + 128]
            run_sum[rows] = total
            run_max[rows] = new
            mixed[rows] = mixed[rows] * factor + jnp.dot(
                weights.astype(BF16), keys, preferred_element_type=F32
            )
        return carry

    lax.fori_loop(0, 8, attention_step, 0)

    for pair in range(2):
        base = pair * 512
        halves = []
        for h in range(2):
            rows = slice(base + h * 256, base + h * 256 + 256)
            halves.append(mixed[rows] / jnp.sum(run_sum[rows], axis=1, keepdims=True))
        attn_ref[:, pair * 128 : pair * 128 + 128] = jnp.where(
            low, pltpu.roll(halves[0], 64, 1), halves[1]
        ).astype(BF16)
    leaving = [pltpu.make_async_copy(attn_ref, attn_out, own_sem.at[5])]
    leaving[0].start()

    for copy in local:
        copy.wait()
    remote(
        send_ref.at[pl.ds(0, N_EP - 1)], arrived.at[pl.ds(0, N_EP - 1)],
        disp_send.at[0], disp_recv.at[0], "ep", up_x,
    ).wait()
    rows_bf[...] = arrived[...].astype(F32).reshape(N_EP * CAP, -1).astype(BF16)

    for slot in range(N_TP):
        if slot == 3:
            for i in range(4):
                complete(i)
        rows_in = rows_bf[...]
        gate = jnp.dot(rows_in, wgb[slot], preferred_element_type=F32)
        up = jnp.dot(rows_in, wub[slot], preferred_element_type=F32)
        hidden[slot] = silu_times(gate, up)

    columns = [pl.ds(first, count) for first, count in CHUNKS]

    def send_back(j):
        def one(i, carry):
            peer = lax.rem(me + i, N_EP)
            remote(
                outbuf.at[peer, :, columns[j]], ret.at[me, :, columns[j]],
                ret_send.at[j], ret_recv.at[j], "ep", peer,
            ).start()
            return carry

        lax.fori_loop(1, N_EP, one, 0)

    back = []
    for j, (first, count) in enumerate(CHUNKS):
        service(4 + j)
        complete(4 + j)
        total = jnp.zeros((N_EP * CAP, count), F32)
        for slot in range(N_TP):
            total = total + jnp.dot(
                hidden[slot], wdb[slot, :, first : first + count], preferred_element_type=F32
            ).astype(BF16).astype(F32)
        outbuf[:, :, first : first + count] = total.reshape(N_EP, CAP, count).astype(BF16)
        send_back(j)
        copy = pltpu.make_async_copy(
            outbuf.at[me, :, columns[j]], ret.at[me, :, columns[j]], own_sem.at[8 + j]
        )
        copy.start()
        back.append(copy)
        if j == 0:
            for b in range(3):
                wide_copy(b, 0).wait_recv()
                wide_copy(b, 2).start()
                pair_copy(b, 2).start()
                wide_copy(b, 1).wait_recv()
                wide_copy(b, 3).start()
                pair_copy(b, 1).start()

    for b in range(3):
        wide_copy(b, 2).wait_recv()
        wide_copy(b, 3).wait_recv()
        pair_copy(b, 3).start()
    for n in range(4):
        for b in range(3):
            pair_copy(b, n).wait_recv()
    shared[...] = jnp.zeros_like(shared)

    def shared_step(slot, carry):
        rows_in = normed_ref[...]
        gate = jnp.dot(rows_in, sgb[slot].reshape(-1, 256), preferred_element_type=F32)
        up = jnp.dot(rows_in, sub[slot].reshape(-1, 256), preferred_element_type=F32)
        units = silu_times(gate, up)
        for n in range(16):
            here = slice(n * 128, n * 128 + 128)
            half = n % 2 * 4
            down = sdb[slot, n // 8, n // 2 % 4, half : half + 4].reshape(256, 128)
            shared[:, here] += jnp.dot(
                units, down, preferred_element_type=F32
            ).astype(BF16).astype(F32)
        return carry

    lax.fori_loop(0, N_TP, shared_step, 0)

    for i in range(len(items)):
        for n in range(4):
            item_copy(i, n).wait_send()
    for i in range(1, N_Z):
        along_z(i).wait_send()
    for copy in (to_next, to_prev, on_next, on_prev):
        copy.wait_send()
    for n in range(4):
        to_core(blocks[n], n).wait_send()
    for b in range(3):
        for slot in range(1, N_TP):
            unit_copy(b, slot).wait_send()
        for step, up in ring_steps:
            ring_copy(b, step, up).wait_send()
        for n in range(4):
            wide_copy(b, n).wait_send()
            pair_copy(b, n).wait_send()

    for j, (first, count) in enumerate(CHUNKS):
        here = slice(first, first + count)
        back[j].wait()
        remote(
            outbuf.at[pl.ds(0, N_EP - 1), :, columns[j]], ret.at[pl.ds(0, N_EP - 1), :, columns[j]],
            ret_send.at[j], ret_recv.at[j], "ep", up_x,
        ).wait()
        flat = ret[:, :, here].astype(F32).reshape(N_EP * CAP, count).astype(BF16)
        total = shared[:, here]
        for k in range(2):
            picked = jnp.dot(choose_ref[k], flat, preferred_element_type=F32)
            total = total + gates_ref[k, :, 0:1] * picked
        moe_ref[:, here] = total.astype(BF16)
        leaving.append(pltpu.make_async_copy(
            moe_ref.at[:, columns[j]], moe_out.at[:, columns[j]], own_sem.at[32 + j]
        ))
        leaving[-1].start()
    for copy in leaving:
        copy.wait()


def layer(tokens, small, weights):
    vmem = pl.BlockSpec(memory_space=pltpu.VMEM)
    anywhere = pl.BlockSpec(memory_space=pl.ANY)
    width = tokens.shape[1]
    dma = pltpu.SemaphoreType.DMA
    return pl.pallas_call(
        layer_kernel,
        out_shape=[
            jax.ShapeDtypeStruct((256, 256), BF16),
            jax.ShapeDtypeStruct(tokens.shape, BF16),
        ],
        in_specs=[vmem] * len(small) + [anywhere] * len(weights),
        out_specs=[anywhere, anywhere],
        scratch_shapes=[
            pltpu.VMEM((256, 256), BF16),
            pltpu.VMEM((128, width), BF16),
            pltpu.VMEM((1024, 128), BF16),
            pltpu.VMEM((128, width), BF16),
            pltpu.VMEM((N_EP, CAP, width), BF16),
            pltpu.VMEM((2, 128, N_EP * CAP), BF16),
            pltpu.VMEM((2, 128, 128), F32),
            pltpu.VMEM((N_CORE, N_X, N_Z, 256, 128), BF16),
            pltpu.VMEM((1024, 128), F32),
            pltpu.VMEM((1024, 128), F32),
            pltpu.VMEM((1024, 128), F32),
            pltpu.VMEM((N_TP, width, 256), BF16),
            pltpu.VMEM((N_TP, width, 256), BF16),
            pltpu.VMEM((N_TP, 256, width), BF16),
            pltpu.VMEM((N_EP, CAP, width), BF16),
            pltpu.VMEM((N_EP * CAP, width), BF16),
            pltpu.VMEM((N_TP, N_EP * CAP, 256), BF16),
            pltpu.VMEM((N_EP, CAP, width), BF16),
            pltpu.VMEM((N_EP, CAP, width), BF16),
            pltpu.VMEM((N_TP, N_CORE, N_X, N_Z, 32, 256), BF16),
            pltpu.VMEM((N_TP, N_CORE, N_X, N_Z, 32, 256), BF16),
            pltpu.VMEM((N_TP, N_CORE, N_X, N_Z, 64, 128), BF16),
            pltpu.VMEM((128, width), F32),
            dma((9, 4)), dma((9, 4)), dma((N_Z,)), dma((N_Z,)), dma((4,)), dma((4,)),
            dma((4,)), dma((4,)), dma((1,)), dma((1,)), dma((len(CHUNKS),)), dma((len(CHUNKS),)),
            dma((3, 4)), dma((3, 4)), dma((3, 8)), dma((3, 8)), dma((3, 4)), dma((3, 4)),
            dma((3, 4)), dma((3, 4)), dma((40,)),
        ],
        compiler_params=pltpu.CompilerParams(
            collective_id=1, has_side_effects=True, vmem_limit_bytes=60 * 1024 * 1024
        ),
        name="layer",
    )(*small, *weights)


def body(
    query_rows, key_rows, value_rows, query_gain, key_gain, moe_tokens, norm_gain, routes,
    route_weights, expert_gate, expert_up, expert_down, shared_gate, shared_up, shared_down,
):
    small = (
        query_rows, key_rows.T, value_rows.T, query_gain[None, :], key_gain[None, :],
        *(jnp.asarray(table) for table in angle_tables()),
        moe_tokens, norm_gain[None, :], routes.T, route_weights.T,
    )
    weights = (
        expert_gate[0], expert_up[0], expert_down[0],
        shared_gate.reshape(N_CORE, N_X, N_Z, 32, 256), shared_up.reshape(N_CORE, N_X, N_Z, 32, 256),
        shared_down.reshape(4, 64, -1),
    )
    return tuple(layer(moe_tokens, small, weights))


def solution(mesh):
    return jax.shard_map(
        body,
        mesh=mesh,
        in_specs=(
            P("ep", "tp"), P("ep", "tp"), P("ep", "tp"), P(), P(),
            P(("ep", "tp"), None), P(), P("ep", None), P("ep", None),
            P("ep", None, "tp"), P("ep", None, "tp"), P("ep", "tp", None),
            P(None, "tp"), P(None, "tp"), P("tp", None),
        ),
        out_specs=(P("ep", "tp"), P(("ep", "tp"), None)),
        check_vma=False,
    )
```

```python
import functools

import jax
import jax.numpy as jnp
import numpy as np
from jax import lax
from jax.experimental import pallas as pl
from jax.experimental.pallas import tpu as pltpu
from jax.sharding import PartitionSpec as P

GRID_W = 64
TOKENS_A = 16384
MESH = pl.DeviceIdType.MESH
F32 = jnp.float32
BF16 = jnp.bfloat16

epsilon = 1e-06
rotary_base = 10000.0
routed_scale = 2.5

N_Z, N_X, N_CORE = 8, 4, 2
N_EP, N_TP = 64, 4
CAP = 8
CHUNKS = ((0, 256), (256, 256), (512, 512), (1024, 512), (1536, 512))
NT = (((1,), (1,)), ((), ()))


def angle_tables():
    pairs = np.arange(128) % 64 // 2
    inv_freq = (rotary_base ** (-np.arange(16, dtype=np.float64) / 16)).astype(np.float32)
    freq = inv_freq[pairs % 16]
    sign = np.where(np.arange(128) % 2 == 0, -1.0, 1.0)
    tables = []
    for count, mask in ((TOKENS_A // GRID_W, pairs < 16), (GRID_W, pairs >= 16)):
        angles = (np.arange(count, dtype=np.float32)[:, None] * freq).astype(np.float64)
        tables.append((np.cos(angles) * mask).astype(np.float32))
        tables.append((np.sin(angles) * sign * mask).astype(np.float32))
    return tables


def silu_times(gate, up):
    return (gate / (1.0 + jnp.exp(-gate)) * up).astype(BF16)


def layer_kernel(
    query_ref, key_ref, value_ref, qgain_ref, kgain_ref, rcos_ref, rsin_ref, ccos_ref, csin_ref,
    tokens_ref, ngain_ref, routes_ref, scores_ref,
    wg_ref, wu_ref, wd_ref, sg_ref, su_ref, sd_ref,
    attn_out, moe_out,
    attn_ref, moe_ref, q_ref, normed_ref, send_ref, choose_ref, gates_ref,
    kvb, run_max, run_sum, mixed,
    wgb, wub, wdb, arrived, rows_bf, hidden, outbuf, ret,
    sgb, sub, sdb, shared,
    item_send, item_recv, kv_send, kv_recv, x_send, x_recv, core_send, core_recv,
    disp_send, disp_recv, ret_send, ret_recv, unit_send, unit_recv, ring_send, ring_recv,
    wide_send, wide_recv, pair_send, pair_recv, own_sem,
):
    me, lane = lax.axis_index("ep"), lax.axis_index("tp")
    z, x, c = lax.div(me, 8), lax.rem(lax.div(me, 2), 4), lax.rem(me, 2)
    right, left = lax.rem(lane + 1, N_TP), lax.rem(lane + 3, N_TP)
    opposite = lax.rem(lane + 2, N_TP)

    def at(zz, xx, cc):
        return (zz * N_X + xx) * N_CORE + cc

    def remote(src, dst, send_sem, recv_sem, axis, peer):
        return pltpu.make_async_remote_copy(
            src_ref=src, dst_ref=dst, send_sem=send_sem, recv_sem=recv_sem,
            device_id={axis: peer}, device_id_type=MESH,
        )

    barrier = pltpu.get_barrier_semaphore()

    def greet(i, carry):
        pl.semaphore_signal(
            barrier, inc=1, device_id={"ep": lax.rem(me + i, N_EP)}, device_id_type=MESH
        )
        return carry

    for i in range(1, N_TP):
        pl.semaphore_signal(
            barrier, inc=1, device_id={"tp": lax.rem(lane + i, N_TP)}, device_id_type=MESH
        )
    lax.fori_loop(1, N_EP, greet, 0)
    pl.semaphore_wait(barrier, N_EP - 1 + N_TP - 1)

    items = []
    for ref, buf in ((wg_ref, wgb), (wu_ref, wub)):
        for h in range(2):
            items.append((ref.at[pl.ds(h * 1024, 1024)], buf, (pl.ds(h * 1024, 1024),), h * 1024, 512))
    for first, count in CHUNKS:
        items.append((wd_ref.at[:, pl.ds(first, count)], wdb, (slice(None), pl.ds(first, count)), 0, 128))

    def item_copy(i, n):
        src, buf, where, base, half = items[i]
        s, r = item_send.at[i], item_recv.at[i]
        lower, upper = pl.ds(base, half), pl.ds(base + half, half)

        def piece(slot, rows):
            return buf.at[(slot, rows) + where[1:]]

        if n == 0:
            return remote(src, buf.at[(1,) + where], s.at[0], r.at[0], "tp", right)
        if n == 1:
            return remote(src, buf.at[(2,) + where], s.at[1], r.at[1], "tp", left)
        if n == 2:
            return remote(piece(1, lower), piece(3, lower), s.at[2], r.at[2], "tp", right)
        return remote(piece(2, upper), piece(3, upper), s.at[3], r.at[3], "tp", left)

    def begin(i):
        item_copy(i, 0).start()
        item_copy(i, 1).start()

    def service(i):
        item_copy(i, 0).wait_recv()
        item_copy(i, 2).start()
        item_copy(i, 1).wait_recv()
        item_copy(i, 3).start()
        for later in follows.get(i, ()):
            begin(later)

    follows = {0: (3,), 3: (4,), 4: (5, 6), 5: (7,), 6: (8,)}

    def complete(i):
        item_copy(i, 2).wait_recv()
        item_copy(i, 3).wait_recv()

    column = pl.ds(pl.multiple_of(((c * N_X + x) * 2 + lax.div(z, 4)) * 128, 128), 128)
    bufs = (sgb, sub, sdb)
    shares = (sg_ref.at[c, x, z], su_ref.at[c, x, z], sd_ref.at[lax.rem(z, 4), :, column])
    others = pl.ds(1, N_TP - 1)

    def unit_copy(b, slot):
        peer = {1: right, 2: left, 3: opposite}[slot]
        return remote(
            shares[b], bufs[b].at[slot, c, x, z], unit_send.at[b, slot], unit_recv.at[b, slot], "tp", peer
        )

    def ring_copy(b, step, up):
        origin = lax.rem(z + (N_Z - step + 1 if up else step - 1), N_Z)
        ref = bufs[b].at[others, c, x, origin]
        n = step - 1 if up else step + 3
        to = lax.rem(z + (1 if up else N_Z - 1), N_Z)
        return remote(ref, ref, ring_send.at[b, n], ring_recv.at[b, n], "ep", at(to, x, c))

    ring_steps = ((1, True), (1, False), (2, True), (2, False), (3, True), (3, False), (4, True))

    def ring_begin(step):
        for b in range(3):
            ring_copy(b, step, True).start()
            if step < 4:
                ring_copy(b, step, False).start()

    def ring_finish(step):
        for b in range(3):
            ring_copy(b, step, True).wait_recv()
            if step < 4:
                ring_copy(b, step, False).wait_recv()

    for slot in range(1, N_TP):
        for b in range(3):
            unit_copy(b, slot).start()
    begin(0)
    begin(1)
    begin(2)

    rows = query_ref.shape[0]
    lanes = lax.broadcasted_iota(jnp.int32, (rows, 128), 1)
    low, even = lanes < 64, lax.rem(lanes, 2) == 0
    grid_rows = rows // GRID_W

    def table(row_ref, col_ref):
        return jnp.concatenate(
            [row_ref[pl.ds(me * grid_rows + n, 1), :] + col_ref[...] for n in range(grid_rows)], axis=0
        )

    cosine, sine = table(rcos_ref, ccos_ref), table(rsin_ref, csin_ref)

    def turned(values, gain):
        squares = values * values
        first = jnp.sum(jnp.where(low, squares, 0.0), axis=1, keepdims=True) / 64.0
        second = jnp.sum(jnp.where(low, 0.0, squares), axis=1, keepdims=True) / 64.0
        inverse = jnp.where(low, lax.rsqrt(first + epsilon), lax.rsqrt(second + epsilon))
        y = values * inverse * gain
        partner = jnp.where(even, pltpu.roll(y, 127, 1), pltpu.roll(y, 1, 1))
        return (y * cosine + partner * sine).astype(BF16).astype(F32)

    def both(gain_ref):
        return jnp.concatenate([gain_ref[...], gain_ref[...]], axis=1)

    kv = jnp.concatenate([key_ref[...].astype(F32), value_ref[...].astype(F32)], axis=0).T
    kvb[c, x, z] = jnp.where(low, turned(kv, both(kgain_ref)), kv).astype(BF16)

    def along_z(i):
        return remote(
            kvb.at[c, x, z], kvb.at[c, x, z], kv_send.at[i], kv_recv.at[i],
            "ep", at(lax.rem(z + i, N_Z), x, c),
        )

    for i in range(1, N_Z):
        along_z(i).start()

    local = []
    for n, (src, dst) in enumerate((
        (wg_ref, wgb.at[0]), (wu_ref, wub.at[0]), (sg_ref, sgb.at[0]), (su_ref, sub.at[0]),
    )):
        local.append(pltpu.make_async_copy(src, dst, own_sem.at[n]))
    local.append(pltpu.make_async_copy(wd_ref, wdb.at[0], own_sem.at[4]))
    for n in range(16):
        local.append(pltpu.make_async_copy(
            sd_ref.at[:, :, pl.ds(n * 128, 128)],
            sdb.at[0, n // 8, n // 2 % 4, pl.ds(n % 2 * 4, 4)], own_sem.at[16 + n],
        ))
    for copy in local:
        copy.start()
    for slot in range(1, N_TP):
        for b in range(3):
            unit_copy(b, slot).wait_recv()
    ring_begin(1)

    gain = both(qgain_ref)
    for pair in range(2):
        values = query_ref[:, pair * 128 : pair * 128 + 128].astype(F32)
        out = turned(values, gain) * 0.125
        base = 2 * pair * rows
        q_ref[base : base + rows, :] = jnp.where(low, out, 0.0).astype(BF16)
        q_ref[base + rows : base + 2 * rows, :] = jnp.where(
            low, pltpu.roll(out, 64, 1), 0.0
        ).astype(BF16)

    values = tokens_ref[...].astype(F32)
    normed_ref[...] = (
        values
        * lax.rsqrt(jnp.mean(values * values, axis=-1, keepdims=True) + epsilon)
        * ngain_ref[...]
    ).astype(BF16)
    own_rows = pl.ds(pl.multiple_of(lane * 128, 128), 128)
    routes = routes_ref[:, own_rows]
    expert_ids = lax.broadcasted_iota(jnp.int32, (N_EP, 128), 0)
    named = [expert_ids == routes[k : k + 1, :] for k in range(2)]
    counts = jnp.where(named[0] | named[1], 1.0, 0.0).astype(BF16)
    square = (128, 128)
    before = jnp.where(
        lax.broadcasted_iota(jnp.int32, square, 0) < lax.broadcasted_iota(jnp.int32, square, 1), 1.0, 0.0
    ).astype(BF16)
    earlier = jnp.dot(counts, before, preferred_element_type=F32)
    slot_ids = lax.broadcasted_iota(jnp.int32, (N_EP * CAP, 128), 0).astype(F32)
    placing = 0.0
    for k in range(2):
        rank = jnp.sum(jnp.where(named[k], earlier, 0.0), axis=0, keepdims=True)
        place = jnp.where(slot_ids == routes[k : k + 1, :].astype(F32) * CAP + rank, 1.0, 0.0)
        placing = placing + place
        choose_ref[k] = place.T.astype(BF16)
    send_ref[...] = jnp.dot(
        placing.astype(BF16), normed_ref[...], preferred_element_type=F32
    ).reshape(N_EP, CAP, -1).astype(BF16)
    scores = scores_ref[:, own_rows]
    gates = scores / (scores[0:1] + scores[1:2]) * routed_scale
    for k in range(2):
        gates_ref[k] = jnp.broadcast_to(gates[k : k + 1], square).T
    arrived[me] = send_ref[me]
    ring_finish(1)
    ring_begin(2)

    x_next, x_prev = lax.rem(x + 1, N_X), lax.rem(x + 3, N_X)
    x_far = lax.rem(x + 2, N_X)
    up_x, down_x = at(z, x_next, c), at(z, x_prev, c)
    low_z, high_z = pl.ds(0, 4), pl.ds(4, 4)
    to_next = remote(kvb.at[c, x], kvb.at[c, x], x_send.at[0], x_recv.at[0], "ep", up_x)
    to_prev = remote(kvb.at[c, x], kvb.at[c, x], x_send.at[1], x_recv.at[1], "ep", down_x)
    on_next = remote(
        kvb.at[c, x_prev, low_z], kvb.at[c, x_prev, low_z], x_send.at[2], x_recv.at[2], "ep", up_x
    )
    on_prev = remote(
        kvb.at[c, x_next, high_z], kvb.at[c, x_next, high_z], x_send.at[3], x_recv.at[3], "ep", down_x
    )

    def to_core(block, n):
        return remote(
            kvb.at[c, block], kvb.at[c, block], core_send.at[n], core_recv.at[n],
            "ep", at(z, x, 1 - c),
        )

    blocks = (x, x_next, x_prev, x_far)

    for i in range(1, N_Z):
        along_z(i).wait_recv()
    to_next.start()
    to_prev.start()
    to_core(blocks[0], 0).start()

    ring_finish(2)
    ring_begin(3)

    def wide_copy(b, n):
        if n < 2:
            ref = bufs[b].at[others, c, x]
        elif n == 2:
            ref = bufs[b].at[others, c, x_prev, low_z]
        else:
            ref = bufs[b].at[others, c, x_next, high_z]
        return remote(ref, ref, wide_send.at[b, n], wide_recv.at[b, n], "ep", (up_x, down_x)[n % 2])

    def pair_copy(b, n):
        ref = bufs[b].at[others, c, blocks[n]]
        return remote(ref, ref, pair_send.at[b, n], pair_recv.at[b, n], "ep", at(z, x, 1 - c))

    def dispatch(i, carry):
        peer = lax.rem(me + i, N_EP)
        remote(
            send_ref.at[peer], arrived.at[me], disp_send.at[0], disp_recv.at[0], "ep", peer
        ).start()
        return carry

    lax.fori_loop(1, 9, dispatch, 0)

    ring_finish(3)
    ring_begin(4)

    lax.fori_loop(9, N_EP, dispatch, 0)

    service(0)

    run_max[...] = jnp.full_like(run_max, -jnp.inf)
    run_sum[...] = jnp.zeros_like(run_sum)
    mixed[...] = jnp.zeros_like(mixed)

    def attention_step(t, carry):
        xi = lax.div(t, 2)
        x_rel = xi + lax.div(xi, 2) - 2 * lax.div(xi, 3)
        block = lax.rem(x + x_rel, N_X)
        core = lax.rem(c + lax.rem(t, 2), N_CORE)

        @pl.when(t == 1)
        def _():
            to_core(blocks[0], 0).wait_recv()

        @pl.when(t == 2)
        def _():
            service(1)
            to_prev.wait_recv()
            on_prev.start()
            to_core(x_next, 1).start()
            to_next.wait_recv()
            on_next.start()
            to_core(x_prev, 2).start()

        @pl.when(t == 3)
        def _():
            to_core(x_next, 1).wait_recv()
            ring_finish(4)
            for b in range(3):
                wide_copy(b, 0).start()
                wide_copy(b, 1).start()
                pair_copy(b, 0).start()

        @pl.when(t == 4)
        def _():
            service(2)

        @pl.when(t == 5)
        def _():
            to_core(x_prev, 2).wait_recv()

        @pl.when(t == 6)
        def _():
            service(3)
            on_next.wait_recv()
            on_prev.wait_recv()
            to_core(x_far, 3).start()

        @pl.when(t == 7)
        def _():
            to_core(x_far, 3).wait_recv()

        keys = kvb[core, block].reshape(N_Z * 256, 128)
        for qb in range(4):
            rows = slice(qb * 256, qb * 256 + 256)
            scores = lax.dot_general(q_ref[rows], keys, NT, preferred_element_type=F32)
            old = run_max[rows]
            new = jnp.maximum(old, jnp.max(scores, axis=1, keepdims=True))
            factor = jnp.exp(old - new)
            weights = jnp.exp(scores - new[:, :1])
            total = run_sum[rows] * factor
            for n in range(N_Z * 256 // 128):
                total = total + weights[:, n * 128 : n * 128 + 128]
            run_sum[rows] = total
            run_max[rows] = new
            mixed[rows] = mixed[rows] * factor + jnp.dot(
                weights.astype(BF16), keys, preferred_element_type=F32
            )
        return carry

    lax.fori_loop(0, 8, attention_step, 0)

    for pair in range(2):
        base = pair * 512
        halves = []
        for h in range(2):
            rows = slice(base + h * 256, base + h * 256 + 256)
            halves.append(mixed[rows] / jnp.sum(run_sum[rows], axis=1, keepdims=True))
        attn_ref[:, pair * 128 : pair * 128 + 128] = jnp.where(
            low, pltpu.roll(halves[0], 64, 1), halves[1]
        ).astype(BF16)
    leaving = [pltpu.make_async_copy(attn_ref, attn_out, own_sem.at[5])]
    leaving[0].start()

    for copy in local:
        copy.wait()
    remote(
        send_ref.at[pl.ds(0, N_EP - 1)], arrived.at[pl.ds(0, N_EP - 1)],
        disp_send.at[0], disp_recv.at[0], "ep", up_x,
    ).wait()
    rows_bf[...] = arrived[...].astype(F32).reshape(N_EP * CAP, -1).astype(BF16)

    for slot in range(N_TP):
        if slot == 3:
            service(4)
            for i in range(4):
                complete(i)
        rows_in = rows_bf[...]
        gate = jnp.dot(rows_in, wgb[slot], preferred_element_type=F32)
        up = jnp.dot(rows_in, wub[slot], preferred_element_type=F32)
        hidden[slot] = silu_times(gate, up)

    columns = [pl.ds(first, count) for first, count in CHUNKS]

    def send_back(j):
        def one(i, carry):
            peer = lax.rem(me + i, N_EP)
            remote(
                outbuf.at[peer, :, columns[j]], ret.at[me, :, columns[j]],
                ret_send.at[j], ret_recv.at[j], "ep", peer,
            ).start()
            return carry

        lax.fori_loop(1, N_EP, one, 0)

    back = []
    for j, (first, count) in enumerate(CHUNKS):
        if j:
            service(4 + j)
        complete(4 + j)
        total = jnp.zeros((N_EP * CAP, count), F32)
        for slot in range(N_TP):
            total = total + jnp.dot(
                hidden[slot], wdb[slot, :, first : first + count], preferred_element_type=F32
            ).astype(BF16).astype(F32)
        outbuf[:, :, first : first + count] = total.reshape(N_EP, CAP, count).astype(BF16)
        send_back(j)
        copy = pltpu.make_async_copy(
            outbuf.at[me, :, columns[j]], ret.at[me, :, columns[j]], own_sem.at[8 + j]
        )
        copy.start()
        back.append(copy)
        for b in {1: (0, 1), 2: (2,)}.get(j, ()):
            wide_copy(b, 0).wait_recv()
            wide_copy(b, 2).start()
            pair_copy(b, 2).start()
            wide_copy(b, 1).wait_recv()
            wide_copy(b, 3).start()
            pair_copy(b, 1).start()

    for b in range(3):
        wide_copy(b, 2).wait_recv()
        wide_copy(b, 3).wait_recv()
        pair_copy(b, 3).start()
    for n in range(4):
        for b in range(3):
            pair_copy(b, n).wait_recv()
    shared[...] = jnp.zeros_like(shared)

    def shared_step(slot, carry):
        rows_in = normed_ref[...]
        gate = jnp.dot(rows_in, sgb[slot].reshape(-1, 256), preferred_element_type=F32)
        up = jnp.dot(rows_in, sub[slot].reshape(-1, 256), preferred_element_type=F32)
        units = silu_times(gate, up)
        for n in range(16):
            here = slice(n * 128, n * 128 + 128)
            half = n % 2 * 4
            down = sdb[slot, n // 8, n // 2 % 4, half : half + 4].reshape(256, 128)
            shared[:, here] += jnp.dot(
                units, down, preferred_element_type=F32
            ).astype(BF16).astype(F32)
        return carry

    lax.fori_loop(0, N_TP, shared_step, 0)

    for i in range(len(items)):
        for n in range(4):
            item_copy(i, n).wait_send()
    for i in range(1, N_Z):
        along_z(i).wait_send()
    for copy in (to_next, to_prev, on_next, on_prev):
        copy.wait_send()
    for n in range(4):
        to_core(blocks[n], n).wait_send()
    for b in range(3):
        for slot in range(1, N_TP):
            unit_copy(b, slot).wait_send()
        for step, up in ring_steps:
            ring_copy(b, step, up).wait_send()
        for n in range(4):
            wide_copy(b, n).wait_send()
            pair_copy(b, n).wait_send()

    for j, (first, count) in enumerate(CHUNKS):
        here = slice(first, first + count)
        back[j].wait()
        remote(
            outbuf.at[pl.ds(0, N_EP - 1), :, columns[j]], ret.at[pl.ds(0, N_EP - 1), :, columns[j]],
            ret_send.at[j], ret_recv.at[j], "ep", up_x,
        ).wait()
        flat = ret[:, :, here].astype(F32).reshape(N_EP * CAP, count).astype(BF16)
        total = shared[:, here]
        for k in range(2):
            picked = jnp.dot(choose_ref[k], flat, preferred_element_type=F32)
            total = total + gates_ref[k, :, 0:1] * picked
        moe_ref[:, here] = total.astype(BF16)
        leaving.append(pltpu.make_async_copy(
            moe_ref.at[:, columns[j]], moe_out.at[:, columns[j]], own_sem.at[32 + j]
        ))
        leaving[-1].start()
    for copy in leaving:
        copy.wait()


def layer(tokens, small, weights):
    vmem = pl.BlockSpec(memory_space=pltpu.VMEM)
    anywhere = pl.BlockSpec(memory_space=pl.ANY)
    width = tokens.shape[1]
    dma = pltpu.SemaphoreType.DMA
    return pl.pallas_call(
        layer_kernel,
        out_shape=[
            jax.ShapeDtypeStruct((256, 256), BF16),
            jax.ShapeDtypeStruct(tokens.shape, BF16),
        ],
        in_specs=[vmem] * len(small) + [anywhere] * len(weights),
        out_specs=[anywhere, anywhere],
        scratch_shapes=[
            pltpu.VMEM((256, 256), BF16),
            pltpu.VMEM((128, width), BF16),
            pltpu.VMEM((1024, 128), BF16),
            pltpu.VMEM((128, width), BF16),
            pltpu.VMEM((N_EP, CAP, width), BF16),
            pltpu.VMEM((2, 128, N_EP * CAP), BF16),
            pltpu.VMEM((2, 128, 128), F32),
            pltpu.VMEM((N_CORE, N_X, N_Z, 256, 128), BF16),
            pltpu.VMEM((1024, 128), F32),
            pltpu.VMEM((1024, 128), F32),
            pltpu.VMEM((1024, 128), F32),
            pltpu.VMEM((N_TP, width, 256), BF16),
            pltpu.VMEM((N_TP, width, 256), BF16),
            pltpu.VMEM((N_TP, 256, width), BF16),
            pltpu.VMEM((N_EP, CAP, width), BF16),
            pltpu.VMEM((N_EP * CAP, width), BF16),
            pltpu.VMEM((N_TP, N_EP * CAP, 256), BF16),
            pltpu.VMEM((N_EP, CAP, width), BF16),
            pltpu.VMEM((N_EP, CAP, width), BF16),
            pltpu.VMEM((N_TP, N_CORE, N_X, N_Z, 32, 256), BF16),
            pltpu.VMEM((N_TP, N_CORE, N_X, N_Z, 32, 256), BF16),
            pltpu.VMEM((N_TP, N_CORE, N_X, N_Z, 64, 128), BF16),
            pltpu.VMEM((128, width), F32),
            dma((9, 4)), dma((9, 4)), dma((N_Z,)), dma((N_Z,)), dma((4,)), dma((4,)),
            dma((4,)), dma((4,)), dma((1,)), dma((1,)), dma((len(CHUNKS),)), dma((len(CHUNKS),)),
            dma((3, 4)), dma((3, 4)), dma((3, 8)), dma((3, 8)), dma((3, 4)), dma((3, 4)),
            dma((3, 4)), dma((3, 4)), dma((40,)),
        ],
        compiler_params=pltpu.CompilerParams(
            collective_id=1, has_side_effects=True, vmem_limit_bytes=60 * 1024 * 1024
        ),
        name="layer",
    )(*small, *weights)


def body(
    query_rows, key_rows, value_rows, query_gain, key_gain, moe_tokens, norm_gain, routes,
    route_weights, expert_gate, expert_up, expert_down, shared_gate, shared_up, shared_down,
):
    small = (
        query_rows, key_rows.T, value_rows.T, query_gain[None, :], key_gain[None, :],
        *(jnp.asarray(table) for table in angle_tables()),
        moe_tokens, norm_gain[None, :], routes.T, route_weights.T,
    )
    weights = (
        expert_gate[0], expert_up[0], expert_down[0],
        shared_gate.reshape(N_CORE, N_X, N_Z, 32, 256), shared_up.reshape(N_CORE, N_X, N_Z, 32, 256),
        shared_down.reshape(4, 64, -1),
    )
    return tuple(layer(moe_tokens, small, weights))


def solution(mesh):
    return jax.shard_map(
        body,
        mesh=mesh,
        in_specs=(
            P("ep", "tp"), P("ep", "tp"), P("ep", "tp"), P(), P(),
            P(("ep", "tp"), None), P(), P("ep", None), P("ep", None),
            P("ep", None, "tp"), P("ep", None, "tp"), P("ep", "tp", None),
            P(None, "tp"), P(None, "tp"), P("tp", None),
        ),
        out_specs=(P("ep", "tp"), P(("ep", "tp"), None)),
        check_vma=False,
    )
```

```python
import functools

import jax
import jax.numpy as jnp
import numpy as np
from jax import lax
from jax.experimental import pallas as pl
from jax.experimental.pallas import tpu as pltpu
from jax.sharding import PartitionSpec as P

GRID_W = 64
TOKENS_A = 16384
MESH = pl.DeviceIdType.MESH
F32 = jnp.float32
BF16 = jnp.bfloat16

epsilon = 1e-06
rotary_base = 10000.0
routed_scale = 2.5

N_Z, N_X, N_CORE = 8, 4, 2
N_EP, N_TP = 64, 4
CAP = 8
CHUNKS = ((0, 256), (256, 256), (512, 512), (1024, 512), (1536, 512))
NT = (((1,), (1,)), ((), ()))


def angle_tables():
    pairs = np.arange(128) % 64 // 2
    inv_freq = (rotary_base ** (-np.arange(16, dtype=np.float64) / 16)).astype(np.float32)
    freq = inv_freq[pairs % 16]
    sign = np.where(np.arange(128) % 2 == 0, -1.0, 1.0)
    tables = []
    for count, mask in ((TOKENS_A // GRID_W, pairs < 16), (GRID_W, pairs >= 16)):
        angles = (np.arange(count, dtype=np.float32)[:, None] * freq).astype(np.float64)
        tables.append((np.cos(angles) * mask).astype(np.float32))
        tables.append((np.sin(angles) * sign * mask).astype(np.float32))
    return tables


def silu_times(gate, up):
    return (gate / (1.0 + jnp.exp(-gate)) * up).astype(BF16)


def layer_kernel(
    query_ref, key_ref, value_ref, qgain_ref, kgain_ref, rcos_ref, rsin_ref, ccos_ref, csin_ref,
    tokens_ref, ngain_ref, routes_ref, scores_ref,
    wg_ref, wu_ref, wd_ref, sg_ref, su_ref, sd_ref,
    attn_out, moe_out,
    attn_ref, moe_ref, q_ref, normed_ref, send_ref, choose_ref, gates_ref,
    kvb, run_max, run_sum, mixed,
    wgb, wub, wdb, arrived, rows_bf, hidden, outbuf, ret,
    sgb, sub, sdb, shared,
    item_send, item_recv, kv_send, kv_recv, x_send, x_recv, core_send, core_recv,
    disp_send, disp_recv, ret_send, ret_recv, unit_send, unit_recv, ring_send, ring_recv,
    wide_send, wide_recv, pair_send, pair_recv, own_sem,
):
    me, lane = lax.axis_index("ep"), lax.axis_index("tp")
    z, x, c = lax.div(me, 8), lax.rem(lax.div(me, 2), 4), lax.rem(me, 2)
    right, left = lax.rem(lane + 1, N_TP), lax.rem(lane + 3, N_TP)
    opposite = lax.rem(lane + 2, N_TP)

    def at(zz, xx, cc):
        return (zz * N_X + xx) * N_CORE + cc

    def remote(src, dst, send_sem, recv_sem, axis, peer):
        return pltpu.make_async_remote_copy(
            src_ref=src, dst_ref=dst, send_sem=send_sem, recv_sem=recv_sem,
            device_id={axis: peer}, device_id_type=MESH,
        )

    barrier = pltpu.get_barrier_semaphore()

    def greet(i, carry):
        pl.semaphore_signal(
            barrier, inc=1, device_id={"ep": lax.rem(me + i, N_EP)}, device_id_type=MESH
        )
        return carry

    for i in range(1, N_TP):
        pl.semaphore_signal(
            barrier, inc=1, device_id={"tp": lax.rem(lane + i, N_TP)}, device_id_type=MESH
        )
    lax.fori_loop(1, N_EP, greet, 0)
    pl.semaphore_wait(barrier, N_EP - 1 + N_TP - 1)

    items = []
    for ref, buf in ((wg_ref, wgb), (wu_ref, wub)):
        for h in range(2):
            items.append((ref.at[pl.ds(h * 1024, 1024)], buf, (pl.ds(h * 1024, 1024),), h * 1024, 512))
    for first, count in CHUNKS:
        items.append((wd_ref.at[:, pl.ds(first, count)], wdb, (slice(None), pl.ds(first, count)), 0, 128))

    def item_copy(i, n):
        src, buf, where, base, half = items[i]
        s, r = item_send.at[i], item_recv.at[i]
        lower, upper = pl.ds(base, half), pl.ds(base + half, half)

        def piece(slot, rows):
            return buf.at[(slot, rows) + where[1:]]

        if n == 0:
            return remote(src, buf.at[(1,) + where], s.at[0], r.at[0], "tp", right)
        if n == 1:
            return remote(src, buf.at[(2,) + where], s.at[1], r.at[1], "tp", left)
        if n == 2:
            return remote(piece(1, lower), piece(3, lower), s.at[2], r.at[2], "tp", right)
        return remote(piece(2, upper), piece(3, upper), s.at[3], r.at[3], "tp", left)

    def begin(i):
        item_copy(i, 0).start()
        item_copy(i, 1).start()

    def service(i):
        item_copy(i, 0).wait_recv()
        item_copy(i, 2).start()
        item_copy(i, 1).wait_recv()
        item_copy(i, 3).start()
        for later in follows.get(i, ()):
            begin(later)

    follows = {0: (3,), 3: (4, 5), 5: (6, 7), 6: (8,)}

    def complete(i):
        item_copy(i, 2).wait_recv()
        item_copy(i, 3).wait_recv()

    column = pl.ds(pl.multiple_of(((c * N_X + x) * 2 + lax.div(z, 4)) * 128, 128), 128)
    bufs = (sgb, sub, sdb)
    shares = (sg_ref.at[c, x, z], su_ref.at[c, x, z], sd_ref.at[lax.rem(z, 4), :, column])
    others = pl.ds(1, N_TP - 1)

    def unit_copy(b, slot):
        peer = {1: right, 2: left, 3: opposite}[slot]
        return remote(
            shares[b], bufs[b].at[slot, c, x, z], unit_send.at[b, slot], unit_recv.at[b, slot], "tp", peer
        )

    def ring_copy(b, step, up):
        origin = lax.rem(z + (N_Z - step + 1 if up else step - 1), N_Z)
        ref = bufs[b].at[others, c, x, origin]
        n = step - 1 if up else step + 3
        to = lax.rem(z + (1 if up else N_Z - 1), N_Z)
        return remote(ref, ref, ring_send.at[b, n], ring_recv.at[b, n], "ep", at(to, x, c))

    ring_steps = ((1, True), (1, False), (2, True), (2, False), (3, True), (3, False), (4, True))

    def ring_begin(step):
        for b in range(3):
            ring_copy(b, step, True).start()
            if step < 4:
                ring_copy(b, step, False).start()

    def ring_finish(step):
        for b in range(3):
            ring_copy(b, step, True).wait_recv()
            if step < 4:
                ring_copy(b, step, False).wait_recv()

    for slot in range(1, N_TP):
        for b in range(3):
            unit_copy(b, slot).start()
    begin(0)
    begin(1)
    begin(2)

    rows = query_ref.shape[0]
    lanes = lax.broadcasted_iota(jnp.int32, (rows, 128), 1)
    low, even = lanes < 64, lax.rem(lanes, 2) == 0
    grid_rows = rows // GRID_W

    def table(row_ref, col_ref):
        return jnp.concatenate(
            [row_ref[pl.ds(me * grid_rows + n, 1), :] + col_ref[...] for n in range(grid_rows)], axis=0
        )

    cosine, sine = table(rcos_ref, ccos_ref), table(rsin_ref, csin_ref)

    def turned(values, gain):
        squares = values * values
        first = jnp.sum(jnp.where(low, squares, 0.0), axis=1, keepdims=True) / 64.0
        second = jnp.sum(jnp.where(low, 0.0, squares), axis=1, keepdims=True) / 64.0
        inverse = jnp.where(low, lax.rsqrt(first + epsilon), lax.rsqrt(second + epsilon))
        y = values * inverse * gain
        partner = jnp.where(even, pltpu.roll(y, 127, 1), pltpu.roll(y, 1, 1))
        return (y * cosine + partner * sine).astype(BF16).astype(F32)

    def both(gain_ref):
        return jnp.concatenate([gain_ref[...], gain_ref[...]], axis=1)

    kv = jnp.concatenate([key_ref[...].astype(F32), value_ref[...].astype(F32)], axis=0).T
    kvb[c, x, z] = jnp.where(low, turned(kv, both(kgain_ref)), kv).astype(BF16)

    def along_z(i):
        return remote(
            kvb.at[c, x, z], kvb.at[c, x, z], kv_send.at[i], kv_recv.at[i],
            "ep", at(lax.rem(z + i, N_Z), x, c),
        )

    for i in range(1, N_Z):
        along_z(i).start()

    local = []
    for n, (src, dst) in enumerate((
        (wg_ref, wgb.at[0]), (wu_ref, wub.at[0]), (sg_ref, sgb.at[0]), (su_ref, sub.at[0]),
    )):
        local.append(pltpu.make_async_copy(src, dst, own_sem.at[n]))
    local.append(pltpu.make_async_copy(wd_ref, wdb.at[0], own_sem.at[4]))
    for n in range(16):
        local.append(pltpu.make_async_copy(
            sd_ref.at[:, :, pl.ds(n * 128, 128)],
            sdb.at[0, n // 8, n // 2 % 4, pl.ds(n % 2 * 4, 4)], own_sem.at[16 + n],
        ))
    for copy in local:
        copy.start()
    for slot in range(1, N_TP):
        for b in range(3):
            unit_copy(b, slot).wait_recv()
    ring_begin(1)

    gain = both(qgain_ref)
    for pair in range(2):
        values = query_ref[:, pair * 128 : pair * 128 + 128].astype(F32)
        out = turned(values, gain) * 0.125
        base = 2 * pair * rows
        q_ref[base : base + rows, :] = jnp.where(low, out, 0.0).astype(BF16)
        q_ref[base + rows : base + 2 * rows, :] = jnp.where(
            low, pltpu.roll(out, 64, 1), 0.0
        ).astype(BF16)

    values = tokens_ref[...].astype(F32)
    normed_ref[...] = (
        values
        * lax.rsqrt(jnp.mean(values * values, axis=-1, keepdims=True) + epsilon)
        * ngain_ref[...]
    ).astype(BF16)
    own_rows = pl.ds(pl.multiple_of(lane * 128, 128), 128)
    routes = routes_ref[:, own_rows]
    expert_ids = lax.broadcasted_iota(jnp.int32, (N_EP, 128), 0)
    named = [expert_ids == routes[k : k + 1, :] for k in range(2)]
    counts = jnp.where(named[0] | named[1], 1.0, 0.0).astype(BF16)
    square = (128, 128)
    before = jnp.where(
        lax.broadcasted_iota(jnp.int32, square, 0) < lax.broadcasted_iota(jnp.int32, square, 1), 1.0, 0.0
    ).astype(BF16)
    earlier = jnp.dot(counts, before, preferred_element_type=F32)
    slot_ids = lax.broadcasted_iota(jnp.int32, (N_EP * CAP, 128), 0).astype(F32)
    placing = 0.0
    for k in range(2):
        rank = jnp.sum(jnp.where(named[k], earlier, 0.0), axis=0, keepdims=True)
        place = jnp.where(slot_ids == routes[k : k + 1, :].astype(F32) * CAP + rank, 1.0, 0.0)
        placing = placing + place
        choose_ref[k] = place.T.astype(BF16)
    send_ref[...] = jnp.dot(
        placing.astype(BF16), normed_ref[...], preferred_element_type=F32
    ).reshape(N_EP, CAP, -1).astype(BF16)
    scores = scores_ref[:, own_rows]
    gates = scores / (scores[0:1] + scores[1:2]) * routed_scale
    for k in range(2):
        gates_ref[k] = jnp.broadcast_to(gates[k : k + 1], square).T
    arrived[me] = send_ref[me]
    ring_finish(1)
    ring_begin(2)

    x_next, x_prev = lax.rem(x + 1, N_X), lax.rem(x + 3, N_X)
    x_far = lax.rem(x + 2, N_X)
    up_x, down_x = at(z, x_next, c), at(z, x_prev, c)
    low_z, high_z = pl.ds(0, 4), pl.ds(4, 4)
    to_next = remote(kvb.at[c, x], kvb.at[c, x], x_send.at[0], x_recv.at[0], "ep", up_x)
    to_prev = remote(kvb.at[c, x], kvb.at[c, x], x_send.at[1], x_recv.at[1], "ep", down_x)
    on_next = remote(
        kvb.at[c, x_prev, low_z], kvb.at[c, x_prev, low_z], x_send.at[2], x_recv.at[2], "ep", up_x
    )
    on_prev = remote(
        kvb.at[c, x_next, high_z], kvb.at[c, x_next, high_z], x_send.at[3], x_recv.at[3], "ep", down_x
    )

    def to_core(block, n):
        return remote(
            kvb.at[c, block], kvb.at[c, block], core_send.at[n], core_recv.at[n],
            "ep", at(z, x, 1 - c),
        )

    blocks = (x, x_next, x_prev, x_far)

    for i in range(1, N_Z):
        along_z(i).wait_recv()
    to_next.start()
    to_prev.start()
    to_core(blocks[0], 0).start()

    ring_finish(2)
    ring_begin(3)

    def wide_copy(b, n):
        if n < 2:
            ref = bufs[b].at[others, c, x]
        elif n == 2:
            ref = bufs[b].at[others, c, x_prev, low_z]
        else:
            ref = bufs[b].at[others, c, x_next, high_z]
        return remote(ref, ref, wide_send.at[b, n], wide_recv.at[b, n], "ep", (up_x, down_x)[n % 2])

    def pair_copy(b, n):
        ref = bufs[b].at[others, c, blocks[n]]
        return remote(ref, ref, pair_send.at[b, n], pair_recv.at[b, n], "ep", at(z, x, 1 - c))

    def dispatch(i, carry):
        peer = lax.rem(me + i, N_EP)
        remote(
            send_ref.at[peer], arrived.at[me], disp_send.at[0], disp_recv.at[0], "ep", peer
        ).start()
        return carry

    lax.fori_loop(1, 9, dispatch, 0)

    ring_finish(3)
    ring_begin(4)

    lax.fori_loop(9, N_EP, dispatch, 0)

    service(0)

    run_max[...] = jnp.full_like(run_max, -jnp.inf)
    run_sum[...] = jnp.zeros_like(run_sum)
    mixed[...] = jnp.zeros_like(mixed)

    def attention_step(t, carry):
        xi = lax.div(t, 2)
        x_rel = xi + lax.div(xi, 2) - 2 * lax.div(xi, 3)
        block = lax.rem(x + x_rel, N_X)
        core = lax.rem(c + lax.rem(t, 2), N_CORE)

        @pl.when(t == 1)
        def _():
            to_core(blocks[0], 0).wait_recv()

        @pl.when(t == 2)
        def _():
            service(1)
            to_prev.wait_recv()
            on_prev.start()
            to_core(x_next, 1).start()
            to_next.wait_recv()
            on_next.start()
            to_core(x_prev, 2).start()

        @pl.when(t == 3)
        def _():
            to_core(x_next, 1).wait_recv()
            ring_finish(4)
            for b in range(3):
                wide_copy(b, 0).start()
                wide_copy(b, 1).start()
                pair_copy(b, 0).start()

        @pl.when(t == 4)
        def _():
            service(2)

        @pl.when(t == 5)
        def _():
            to_core(x_prev, 2).wait_recv()

        @pl.when(t == 6)
        def _():
            service(3)
            on_next.wait_recv()
            on_prev.wait_recv()
            to_core(x_far, 3).start()

        @pl.when(t == 7)
        def _():
            to_core(x_far, 3).wait_recv()

        keys = kvb[core, block].reshape(N_Z * 256, 128)
        for qb in range(4):
            rows = slice(qb * 256, qb * 256 + 256)
            scores = lax.dot_general(q_ref[rows], keys, NT, preferred_element_type=F32)
            old = run_max[rows]
            new = jnp.maximum(old, jnp.max(scores, axis=1, keepdims=True))
            factor = jnp.exp(old - new)
            weights = jnp.exp(scores - new[:, :1])
            total = run_sum[rows] * factor
            for n in range(N_Z * 256 // 128):
                total = total + weights[:, n * 128 : n * 128 + 128]
            run_sum[rows] = total
            run_max[rows] = new
            mixed[rows] = mixed[rows] * factor + jnp.dot(
                weights.astype(BF16), keys, preferred_element_type=F32
            )
        return carry

    lax.fori_loop(0, 8, attention_step, 0)

    for pair in range(2):
        base = pair * 512
        halves = []
        for h in range(2):
            rows = slice(base + h * 256, base + h * 256 + 256)
            halves.append(mixed[rows] / jnp.sum(run_sum[rows], axis=1, keepdims=True))
        attn_ref[:, pair * 128 : pair * 128 + 128] = jnp.where(
            low, pltpu.roll(halves[0], 64, 1), halves[1]
        ).astype(BF16)
    leaving = [pltpu.make_async_copy(attn_ref, attn_out, own_sem.at[5])]
    leaving[0].start()

    for copy in local:
        copy.wait()
    remote(
        send_ref.at[pl.ds(0, N_EP - 1)], arrived.at[pl.ds(0, N_EP - 1)],
        disp_send.at[0], disp_recv.at[0], "ep", up_x,
    ).wait()
    rows_bf[...] = arrived[...].astype(F32).reshape(N_EP * CAP, -1).astype(BF16)

    for slot in range(N_TP):
        if slot == 3:
            service(4)
            service(5)
            for i in range(4):
                complete(i)
        rows_in = rows_bf[...]
        gate = jnp.dot(rows_in, wgb[slot], preferred_element_type=F32)
        up = jnp.dot(rows_in, wub[slot], preferred_element_type=F32)
        hidden[slot] = silu_times(gate, up)

    columns = [pl.ds(first, count) for first, count in CHUNKS]

    def send_back(j):
        def one(i, carry):
            peer = lax.rem(me + i, N_EP)
            remote(
                outbuf.at[peer, :, columns[j]], ret.at[me, :, columns[j]],
                ret_send.at[j], ret_recv.at[j], "ep", peer,
            ).start()
            return carry

        lax.fori_loop(1, N_EP, one, 0)

    back = []
    for j, (first, count) in enumerate(CHUNKS):
        if j > 1:
            service(4 + j)
        complete(4 + j)
        total = jnp.zeros((N_EP * CAP, count), F32)
        for slot in range(N_TP):
            total = total + jnp.dot(
                hidden[slot], wdb[slot, :, first : first + count], preferred_element_type=F32
            ).astype(BF16).astype(F32)
        outbuf[:, :, first : first + count] = total.reshape(N_EP, CAP, count).astype(BF16)
        send_back(j)
        copy = pltpu.make_async_copy(
            outbuf.at[me, :, columns[j]], ret.at[me, :, columns[j]], own_sem.at[8 + j]
        )
        copy.start()
        back.append(copy)
        for b in {1: (0, 1), 2: (2,)}.get(j, ()):
            wide_copy(b, 0).wait_recv()
            wide_copy(b, 2).start()
            pair_copy(b, 2).start()
            wide_copy(b, 1).wait_recv()
            wide_copy(b, 3).start()
            pair_copy(b, 1).start()

    for b in range(3):
        wide_copy(b, 2).wait_recv()
        wide_copy(b, 3).wait_recv()
        pair_copy(b, 3).start()
    for n in range(4):
        for b in range(3):
            pair_copy(b, n).wait_recv()
    shared[...] = jnp.zeros_like(shared)

    def shared_step(slot, carry):
        rows_in = normed_ref[...]
        gate = jnp.dot(rows_in, sgb[slot].reshape(-1, 256), preferred_element_type=F32)
        up = jnp.dot(rows_in, sub[slot].reshape(-1, 256), preferred_element_type=F32)
        units = silu_times(gate, up)
        for n in range(16):
            here = slice(n * 128, n * 128 + 128)
            half = n % 2 * 4
            down = sdb[slot, n // 8, n // 2 % 4, half : half + 4].reshape(256, 128)
            shared[:, here] += jnp.dot(
                units, down, preferred_element_type=F32
            ).astype(BF16).astype(F32)
        return carry

    lax.fori_loop(0, N_TP, shared_step, 0)

    for i in range(len(items)):
        for n in range(4):
            item_copy(i, n).wait_send()
    for i in range(1, N_Z):
        along_z(i).wait_send()
    for copy in (to_next, to_prev, on_next, on_prev):
        copy.wait_send()
    for n in range(4):
        to_core(blocks[n], n).wait_send()
    for b in range(3):
        for slot in range(1, N_TP):
            unit_copy(b, slot).wait_send()
        for step, up in ring_steps:
            ring_copy(b, step, up).wait_send()
        for n in range(4):
            wide_copy(b, n).wait_send()
            pair_copy(b, n).wait_send()

    for j, (first, count) in enumerate(CHUNKS):
        here = slice(first, first + count)
        back[j].wait()
        remote(
            outbuf.at[pl.ds(0, N_EP - 1), :, columns[j]], ret.at[pl.ds(0, N_EP - 1), :, columns[j]],
            ret_send.at[j], ret_recv.at[j], "ep", up_x,
        ).wait()
        flat = ret[:, :, here].astype(F32).reshape(N_EP * CAP, count).astype(BF16)
        total = shared[:, here]
        for k in range(2):
            picked = jnp.dot(choose_ref[k], flat, preferred_element_type=F32)
            total = total + gates_ref[k, :, 0:1] * picked
        moe_ref[:, here] = total.astype(BF16)
        leaving.append(pltpu.make_async_copy(
            moe_ref.at[:, columns[j]], moe_out.at[:, columns[j]], own_sem.at[32 + j]
        ))
        leaving[-1].start()
    for copy in leaving:
        copy.wait()


def layer(tokens, small, weights):
    vmem = pl.BlockSpec(memory_space=pltpu.VMEM)
    anywhere = pl.BlockSpec(memory_space=pl.ANY)
    width = tokens.shape[1]
    dma = pltpu.SemaphoreType.DMA
    return pl.pallas_call(
        layer_kernel,
        out_shape=[
            jax.ShapeDtypeStruct((256, 256), BF16),
            jax.ShapeDtypeStruct(tokens.shape, BF16),
        ],
        in_specs=[vmem] * len(small) + [anywhere] * len(weights),
        out_specs=[anywhere, anywhere],
        scratch_shapes=[
            pltpu.VMEM((256, 256), BF16),
            pltpu.VMEM((128, width), BF16),
            pltpu.VMEM((1024, 128), BF16),
            pltpu.VMEM((128, width), BF16),
            pltpu.VMEM((N_EP, CAP, width), BF16),
            pltpu.VMEM((2, 128, N_EP * CAP), BF16),
            pltpu.VMEM((2, 128, 128), F32),
            pltpu.VMEM((N_CORE, N_X, N_Z, 256, 128), BF16),
            pltpu.VMEM((1024, 128), F32),
            pltpu.VMEM((1024, 128), F32),
            pltpu.VMEM((1024, 128), F32),
            pltpu.VMEM((N_TP, width, 256), BF16),
            pltpu.VMEM((N_TP, width, 256), BF16),
            pltpu.VMEM((N_TP, 256, width), BF16),
            pltpu.VMEM((N_EP, CAP, width), BF16),
            pltpu.VMEM((N_EP * CAP, width), BF16),
            pltpu.VMEM((N_TP, N_EP * CAP, 256), BF16),
            pltpu.VMEM((N_EP, CAP, width), BF16),
            pltpu.VMEM((N_EP, CAP, width), BF16),
            pltpu.VMEM((N_TP, N_CORE, N_X, N_Z, 32, 256), BF16),
            pltpu.VMEM((N_TP, N_CORE, N_X, N_Z, 32, 256), BF16),
            pltpu.VMEM((N_TP, N_CORE, N_X, N_Z, 64, 128), BF16),
            pltpu.VMEM((128, width), F32),
            dma((9, 4)), dma((9, 4)), dma((N_Z,)), dma((N_Z,)), dma((4,)), dma((4,)),
            dma((4,)), dma((4,)), dma((1,)), dma((1,)), dma((len(CHUNKS),)), dma((len(CHUNKS),)),
            dma((3, 4)), dma((3, 4)), dma((3, 8)), dma((3, 8)), dma((3, 4)), dma((3, 4)),
            dma((3, 4)), dma((3, 4)), dma((40,)),
        ],
        compiler_params=pltpu.CompilerParams(
            collective_id=1, has_side_effects=True, vmem_limit_bytes=60 * 1024 * 1024
        ),
        name="layer",
    )(*small, *weights)


def body(
    query_rows, key_rows, value_rows, query_gain, key_gain, moe_tokens, norm_gain, routes,
    route_weights, expert_gate, expert_up, expert_down, shared_gate, shared_up, shared_down,
):
    small = (
        query_rows, key_rows.T, value_rows.T, query_gain[None, :], key_gain[None, :],
        *(jnp.asarray(table) for table in angle_tables()),
        moe_tokens, norm_gain[None, :], routes.T, route_weights.T,
    )
    weights = (
        expert_gate[0], expert_up[0], expert_down[0],
        shared_gate.reshape(N_CORE, N_X, N_Z, 32, 256), shared_up.reshape(N_CORE, N_X, N_Z, 32, 256),
        shared_down.reshape(4, 64, -1),
    )
    return tuple(layer(moe_tokens, small, weights))


def solution(mesh):
    return jax.shard_map(
        body,
        mesh=mesh,
        in_specs=(
            P("ep", "tp"), P("ep", "tp"), P("ep", "tp"), P(), P(),
            P(("ep", "tp"), None), P(), P("ep", None), P("ep", None),
            P("ep", None, "tp"), P("ep", None, "tp"), P("ep", "tp", None),
            P(None, "tp"), P(None, "tp"), P("tp", None),
        ),
        out_specs=(P("ep", "tp"), P(("ep", "tp"), None)),
        check_vma=False,
    )
```
